256 devices in a mesh: dp: 4 (over x), kv: 32 (over z, y), tp: 2 (over core).
Axes of the slice: x: 4, y: 4, z: 8, core: 2. Of those that a mesh axis runs over, the one named last changes fastest.
Arguments:
- tokens: bfloat16 [128, 4, 2048], P('dp', None, 'kv'), may hold values from -6 to 6
- in_gain: float32 [2048], P('kv'), may hold values from 0.1 to 1.9
- w_gate: bfloat16 [2048, 2048], P('kv', 'tp'), may hold values from -0.125 to 0.125
- w_value: bfloat16 [2048, 2048], P('kv', 'tp'), may hold values from -0.125 to 0.125
- w_key: bfloat16 [2048, 512], P('kv', 'tp'), may hold values from -0.125 to 0.125
- w_query: bfloat16 [2048, 512], P('kv', 'tp'), may hold values from -0.125 to 0.125
- w_step: bfloat16 [2048, 32], P('kv', 'tp'), may hold values from -0.125 to 0.125
- conv_value: bfloat16 [4, 2048], P(None, 'tp'), may hold values from -3 to 3
- conv_key: bfloat16 [4, 512], P(None, 'tp'), may hold values from -3 to 3
- conv_query: bfloat16 [4, 512], P(None, 'tp'), may hold values from -3 to 3
- step_bias: float32 [32], P('tp'), may hold values from -3 to 0
- decay_log: float32 [32], P('tp'), may hold values from -1 to 1.5
- out_gain: float32 [2048], P('tp'), may hold values from 0.1 to 1.9
- w_out: bfloat16 [2048, 2048], P('tp', 'kv'), may hold values from -0.125 to 0.125
- past_value: bfloat16 [128, 7, 2048], P(('dp', 'kv'), None, 'tp'), may hold values from -6 to 6
- past_key: bfloat16 [128, 7, 512], P(('dp', 'kv'), None, 'tp'), may hold values from -6 to 6
- past_query: bfloat16 [128, 7, 512], P(('dp', 'kv'), None, 'tp'), may hold values from -6 to 6
- past_states: float32 [128, 5, 32, 64, 128], P(('dp', 'kv'), None, 'tp'), may hold values from -2 to 2
- accepted: int32 [128], P(('dp', 'kv')), may hold values from 0 to 4
Outputs:
- mixed: bfloat16 [128, 4, 2048], P('dp', None, 'kv')
- new_states: float32 [128, 5, 32, 64, 128], P(('dp', 'kv'), None, 'tp')
- new_value: bfloat16 [128, 7, 2048], P(('dp', 'kv'), None, 'tp')
- new_key: bfloat16 [128, 7, 512], P(('dp', 'kv'), None, 'tp')
- new_query: bfloat16 [128, 7, 512], P(('dp', 'kv'), None, 'tp')
The draws below stay inside these ranges and needn't reach their ends.
All inputs are finite; a program needn't handle non-finite values.
Results may differ from the reference program's by a relative error of at most 0.014.
Values may be sent and summed in bfloat16 or wider, within the bound.
No kernel may reach another device: no remote copies, remote signals or barrier semaphores. Data moves between devices by JAX's collectives and lax.ppermute only.
A program may use at most 64 MiB of HBM per device.

```python
import jax
import jax.numpy as jnp
from jax import lax

D = 2048
HEADS = 32
HEAD_DIM = 64
GROUPS = 4
STATE = 128
CONV = 4
PROP = 4
WIDTH = 2048
KEEP = 5
LAG = 7
SEQS = 128
N_TP = 2


def place_ends(values, key, low, largest):
    extent = values.shape
    index_at = [jax.random.randint(jax.random.fold_in(key, axis), (), 0, extent[axis]) for axis in range(len(extent))]
    values = values.at[tuple(index_at)].set(low)
    longest = extent.index(max(extent))
    index_at[longest] = (index_at[longest] + 1) % extent[longest]
    return values.at[tuple(index_at)].set(largest)


def steps_of(own_key, extent, cuts, least, high):
    factor_of = 1.0
    for dim, shards_of in cuts:
        heights = jax.random.uniform(jax.random.fold_in(jax.random.fold_in(own_key, 6), dim), (shards_of,), jnp.float32, least / len(cuts), high / len(cuts))
        factor_of = factor_of * jnp.repeat(jnp.exp(heights), extent[dim] // shards_of).reshape((-1,) + (1,) * (len(extent) - 1 - dim))
    return factor_of


def centred(rng, dims, deviation, reach, pieces=(), kind=jnp.bfloat16):
    array = deviation * jax.random.normal(rng, dims, jnp.float32)
    if pieces:
        array = array * steps_of(rng, dims, pieces, -0.22, 0.18)
    return jnp.clip(array, -reach, reach).astype(kind)


def setup_inputs(seed: int = 0) -> dict:
    splits = jax.random.split(jax.random.key(seed), 20)
    return {
        "tokens": centred(splits[0], (SEQS, PROP, D), 1.0, 6.0, ((0, 4), (2, 32))),
        "in_gain": jnp.clip(1.0 + 0.18 * jax.random.normal(splits[1], (D,), jnp.float32), 0.1, 1.9),
        "w_gate": centred(splits[2], (D, WIDTH), D ** -0.5, 0.125, ((0, 32), (1, 2))),
        "w_value": centred(splits[3], (D, WIDTH), D ** -0.5, 0.125, ((0, 32), (1, 2))),
        "w_key": centred(splits[4], (D, GROUPS * STATE), D ** -0.5, 0.125, ((0, 32), (1, 2))),
        "w_query": centred(splits[5], (D, GROUPS * STATE), D ** -0.5, 0.125, ((0, 32), (1, 2))),
        "w_step": centred(splits[6], (D, HEADS), D ** -0.5, 0.125, ((0, 32), (1, 2))),
        "conv_value": centred(splits[7], (CONV, WIDTH), 0.5, 3.0, ((1, 2),)),
        "conv_key": centred(splits[8], (CONV, GROUPS * STATE), 0.5, 3.0, ((1, 2),)),
        "conv_query": centred(splits[9], (CONV, GROUPS * STATE), 0.5, 3.0, ((1, 2),)),
        "step_bias": jnp.clip(-3.0 + 3.0 * jax.random.uniform(splits[10], (HEADS,), jnp.float32) ** steps_of(splits[10], (HEADS,), ((0, 2),), -0.2, 0.2), -3.0, 0.0),
        "decay_log": jnp.clip(-1.0 + 2.5 * jax.random.uniform(splits[11], (HEADS,), jnp.float32) ** steps_of(splits[11], (HEADS,), ((0, 2),), -0.2, 0.2), -1.0, 1.5),
        "out_gain": jnp.clip(1.0 + 0.18 * jax.random.normal(splits[12], (WIDTH,), jnp.float32), 0.1, 1.9),
        "w_out": centred(splits[13], (WIDTH, D), WIDTH ** -0.5, 0.125, ((0, 2), (1, 32))),
        "past_value": centred(splits[14], (SEQS, LAG, WIDTH), 1.0, 6.0, ((0, 128), (2, 2))),
        "past_key": centred(splits[15], (SEQS, LAG, GROUPS * STATE), 1.0, 6.0, ((0, 128), (2, 2))),
        "past_query": centred(splits[16], (SEQS, LAG, GROUPS * STATE), 1.0, 6.0, ((0, 128), (2, 2))),
        "past_states": centred(splits[17], (SEQS, KEEP, HEADS, HEAD_DIM, STATE), 0.3, 2.0, ((0, 128), (2, 2)), jnp.float32),
        "accepted": place_ends(jax.random.randint(splits[18], (SEQS,), 0, PROP + 1), jax.random.fold_in(splits[18], 1), 0, PROP).astype(jnp.int32),
    }


EPS = 1e-05

def take_window(history, offsets, span):
    return jax.vmap(lambda rows_one, offset: lax.dynamic_slice_in_dim(rows_one, offset, span, 0))(history, offsets.astype(jnp.int32))

def depthwise(history, taps, proposals):
    total = history[:, 0:proposals].astype(jnp.float32) * taps[0].astype(jnp.float32)
    for offset in range(1, taps.shape[0]):
        total = total + history[:, offset:offset + proposals].astype(jnp.float32) * taps[offset].astype(jnp.float32)
    return jax.nn.silu(total)

def run_chain(values, keys, queries, steps, rates, initial, groups):
    seq_count, proposals, heads = steps.shape
    per_group = heads // groups
    head_dim = values.shape[2] // heads
    state_dim = keys.shape[2] // groups
    carried = initial.reshape(seq_count, groups, per_group, head_dim, state_dim)
    factor = jnp.exp(steps * rates)
    outputs = []
    saved = [initial]
    for position in range(proposals):
        moved = values[:, position].reshape(seq_count, groups, per_group, head_dim) * steps[:, position].reshape(seq_count, groups, per_group)[..., None]
        key_row = keys[:, position].reshape(seq_count, groups, state_dim)
        carried = carried * factor[:, position].reshape(seq_count, groups, per_group)[..., None, None] + moved[..., None] * key_row[:, :, None, None, :]
        query_row = queries[:, position].reshape(seq_count, groups, state_dim)
        result = jnp.einsum('sgrpn,sgn->sgrp', carried, query_row, precision=lax.Precision.HIGHEST)
        outputs.append(result.reshape(seq_count, heads * head_dim))
        saved.append(carried.reshape(seq_count, heads, head_dim, state_dim))
    return (jnp.stack(outputs, 1), jnp.stack(saved, 1))

def reference(tokens, in_gain, w_gate, w_value, w_key, w_query, w_step, conv_value, conv_key, conv_query, step_bias, decay_log, out_gain, w_out, past_value, past_key, past_query, past_states, accepted):
    seq_count, proposals, features = tokens.shape
    widened = tokens.astype(jnp.float32)
    rscale = lax.rsqrt(lax.optimization_barrier(jnp.mean(widened * widened, axis=-1, keepdims=True)) + EPS)
    normed = (widened * in_gain).astype(jnp.bfloat16).reshape(seq_count * proposals, features)

    def project(weight):
        return jnp.dot(normed, weight, preferred_element_type=jnp.float32).reshape(seq_count, proposals, -1) * rscale
    raw_step = project(w_step)
    gate = project(w_gate).astype(jnp.bfloat16)
    value = project(w_value).astype(jnp.bfloat16)
    key = project(w_key).astype(jnp.bfloat16)
    query = project(w_query).astype(jnp.bfloat16)
    span = CONV - 1
    new_value = jnp.concatenate([take_window(past_value, accepted, span), value], axis=1)
    new_key = jnp.concatenate([take_window(past_key, accepted, span), key], axis=1)
    new_query = jnp.concatenate([take_window(past_query, accepted, span), query], axis=1)
    conv_v = depthwise(new_value, conv_value, proposals)
    conv_k = depthwise(new_key, conv_key, proposals)
    conv_q = depthwise(new_query, conv_query, proposals)
    steps = jax.nn.softplus(raw_step + step_bias)
    rates = -jnp.exp(decay_log)
    initial = jnp.take_along_axis(past_states, accepted.astype(jnp.int32)[:, None, None, None, None], axis=1)[:, 0]
    mixed_heads, new_states = run_chain(conv_v, conv_k, conv_q, steps, rates, initial, GROUPS)
    gated = mixed_heads * jax.nn.silu(gate.astype(jnp.float32))
    scale_out = lax.rsqrt(lax.optimization_barrier(jnp.mean(gated * gated, axis=-1, keepdims=True)) + EPS)
    outn = (gated * scale_out * out_gain).astype(jnp.bfloat16).reshape(seq_count * proposals, -1)
    block_width = outn.shape[1] // N_TP
    total = jnp.zeros((seq_count * proposals, features), jnp.float32)
    for block_index in range(N_TP):
        piece = outn[:, block_index * block_width:(block_index + 1) * block_width]
        weight_rows = w_out[block_index * block_width:(block_index + 1) * block_width]
        partial_sum = jnp.dot(piece, weight_rows, preferred_element_type=jnp.float32).astype(jnp.bfloat16)
        total = total + partial_sum.astype(jnp.float32)
    mixed = total.astype(jnp.bfloat16).reshape(seq_count, proposals, features)
    return (mixed, new_states, new_value, new_key, new_query)
```

```python
import jax
import jax.numpy as jnp
from jax import lax
from jax.experimental import pallas as pl
from jax.experimental.pallas import tpu as pltpu
from jax.sharding import PartitionSpec as P

D = 2048
CONV = 4
WIDTH = 2048
EPS = 1e-05

F32 = jnp.float32
BF16 = jnp.bfloat16
LANES = 128
VMEM = pltpu.VMEM
NT = (((1,), (1,)), ((), ()))


def local(x):
    return pltpu.with_memory_space_constraint(x, VMEM)


def lane_of(shape):
    return lax.broadcasted_iota(jnp.int32, shape, 1)


def halves(x):
    high = x.astype(BF16).astype(F32)
    return high, x - high


def project_kernel(tok, gain, wg, wv, wk, wq, ws, out, x_s, ws_s):
    seqs, prop, _ = tok.shape
    for i in range(seqs):
        x_s[prop * i : prop * (i + 1), :] = tok[i].astype(F32)
    ws_s[...] = jnp.zeros(ws_s.shape, BF16)
    ws_s[: ws.shape[0], :] = ws[...]
    x = x_s[...]
    squares = jnp.sum(x * x, axis=1, keepdims=True)
    normed = (x * gain[...]).astype(BF16)

    def put(at, product):
        width = product.shape[1]
        for i in range(seqs):
            out[i, :, at : at + width] = product[prop * i : prop * (i + 1)].astype(BF16)

    at = 0
    for w in (wg, wv, wk, wq):
        for c in range(0, w.shape[1], 256):
            put(at, jnp.dot(normed, w[:, c : c + 256], preferred_element_type=F32))
            at += 256
    heads = ws.shape[0]
    extra = lax.dot_general(normed, ws_s[...], NT, preferred_element_type=F32)
    high, low = halves(squares)
    lane = lane_of(extra.shape)
    extra = jnp.where(lane == heads, high, jnp.where(lane == heads + 1, low, extra))
    put(at, extra)


def project(tokens, gain, weights):
    seqs, prop, feat = tokens.shape
    columns = sum(w.shape[1] for w in weights[:4]) + LANES
    return pl.pallas_call(
        project_kernel,
        out_specs=pl.BlockSpec(memory_space=VMEM),
        out_shape=VMEM((seqs, prop, columns), BF16),
        scratch_shapes=[VMEM((seqs * prop, feat), F32), VMEM((LANES, feat), BF16)],
        name="project",
    )(tokens, gain.reshape(1, feat), *weights[:4], weights[4].T)


def prepare_kernel(
    accepted,
    states,
    past_v,
    past_k,
    past_q,
    taps_v,
    taps_k,
    taps_q,
    bias,
    log_rate,
    out_gain,
    state,
    state_high,
    state_low,
    rows,
    base,
    taps,
    bias_out,
    rate,
    gain,
    sem,
):
    offset = accepted[0]
    fetch = pltpu.make_async_copy(states.at[0, pl.ds(offset, 1)], state, sem)
    fetch.start()
    span, prop = rows.shape[0], base.shape[0]
    at = 0
    for past, tap in ((past_v, taps_v), (past_k, taps_k), (past_q, taps_q)):
        width = past.shape[2]
        history = past[0].astype(F32)
        picked = history[0:span]
        for j in range(1, history.shape[0] - span + 1):
            picked = jnp.where(offset == j, history[j : j + span], picked)
        weight = tap[...].astype(F32)
        rows[:, at : at + width] = picked
        taps[:, at : at + width] = weight
        for t in range(prop):
            part = jnp.zeros((1, width), F32)
            for i in range(CONV):
                if t + i < span:
                    part = part + picked[t + i : t + i + 1] * weight[i : i + 1]
            base[t : t + 1, at : at + width] = part
        at += width
    bias_out[...] = bias[...]
    rate[...] = -jnp.exp(log_rate[...])
    gain[...] = out_gain[...]
    fetch.wait()
    for h in range(state.shape[1]):
        at = slice(h * state.shape[2], (h + 1) * state.shape[2])
        high = state[0, h].astype(BF16)
        state_high[at] = high
        state_low[at] = (state[0, h] - high.astype(F32)).astype(BF16)


def prepare(accepted, states, pasts, taps, bias, log_rate, out_gain):
    _, _, heads, head_dim, state_dim = states.shape
    inner = heads * head_dim
    width = sum(p.shape[2] for p in pasts)
    prop = pasts[0].shape[1] - (CONV - 1)
    plain, vmem = pl.BlockSpec(), pl.BlockSpec(memory_space=VMEM)
    return pl.pallas_call(
        prepare_kernel,
        in_specs=[pl.BlockSpec(memory_space=pltpu.SMEM), pl.BlockSpec(memory_space=pl.ANY), *[plain] * 9],
        out_specs=[vmem] * 9,
        out_shape=[
            VMEM((1, heads, head_dim, state_dim), F32),
            VMEM((inner, state_dim), BF16),
            VMEM((inner, state_dim), BF16),
            VMEM((CONV - 1, width), F32),
            VMEM((prop, width), F32),
            VMEM((CONV, width), F32),
            VMEM((1, heads), F32),
            VMEM((1, heads), F32),
            VMEM((1, inner), F32),
        ],
        scratch_shapes=[pltpu.SemaphoreType.DMA(())],
        name="prepare",
    )(
        accepted,
        states,
        *pasts,
        *taps,
        bias.reshape(1, heads),
        log_rate.reshape(1, heads),
        out_gain.reshape(1, inner),
    )


def chain_kernel(
    arrived, state_high, state_low, base, taps, bias, rate, gain, sent, moved_out, key_out, decay_out, new_out
):
    copies, prop, _ = arrived.shape
    inner, state_dim = state_high.shape
    heads = bias.shape[1]
    head_dim = inner // heads
    width = base.shape[1]
    kwidth = (width - inner) // 2
    groups = kwidth // state_dim
    per_group = inner // groups

    total = arrived[0].astype(F32)
    for i in range(1, copies):
        total = total + arrived[i].astype(F32)
    at_step = inner + width
    squares = total[:, at_step + heads : at_step + heads + 1] + total[:, at_step + heads + 1 : at_step + heads + 2]
    rscale = lax.rsqrt(squares / D + EPS)

    def scaled(start, stop):
        return (total[:, start:stop] * rscale).astype(BF16).astype(F32)

    new = scaled(inner, at_step)
    new_out[...] = new
    filtered = base[...] + new * taps[CONV - 1 : CONV]
    for i in range(1, CONV):
        later = jnp.concatenate([jnp.zeros((i, width), F32), new[: prop - i]], axis=0)
        filtered = filtered + later * taps[CONV - 1 - i : CONV - i]
    convolved = filtered / (1.0 + jnp.exp(-filtered))
    conv_v, conv_k, conv_q = convolved[:, :inner], convolved[:, inner : inner + kwidth], convolved[:, inner + kwidth :]

    raw = total[:, at_step : at_step + heads] * rscale + bias[...]
    steps = jnp.maximum(raw, 0.0) + jnp.log1p(jnp.exp(-jnp.abs(raw)))
    decay = jnp.exp(steps * rate[...])
    first_half = lane_of((prop, 2 * head_dim)) < head_dim

    def spread(x):
        return jnp.concatenate(
            [jnp.where(first_half, x[:, h : h + 1], x[:, h + 1 : h + 2]) for h in range(0, heads, 2)], axis=1
        )

    moved = spread(steps) * conv_v
    shrink = spread(decay)
    moved_out[0:prop, :] = moved
    moved_out[prop:, :] = jnp.zeros((moved_out.shape[0] - prop, inner), F32)
    key_out[...] = conv_k
    decay_out[...] = decay

    q_high, q_low = halves(conv_q)
    q_both = jnp.concatenate([q_high, q_low], axis=0).astype(BF16)
    row = lax.broadcasted_iota(jnp.int32, (prop, per_group), 0)
    ys = []
    for g in range(groups):
        cols = slice(g * per_group, (g + 1) * per_group)
        part = slice(g * state_dim, (g + 1) * state_dim)
        main = lax.dot_general(q_both[:, part], state_high[cols], NT, preferred_element_type=F32)
        rest = lax.dot_general(q_both[:prop, part], state_low[cols], NT, preferred_element_type=F32)
        carried = main[:prop] + main[prop:] + rest
        y = jnp.zeros((prop, per_group), F32)
        for t in range(prop):
            match = jnp.sum(conv_q[:, part] * conv_k[t : t + 1, part], axis=1, keepdims=True)
            carried = carried * shrink[t : t + 1, cols] + moved[t : t + 1, cols] * match
            y = jnp.where(row == t, carried, y)
        ys.append(y)
    y = jnp.concatenate(ys, axis=1)
    gate = scaled(0, inner)
    u = (y * (gate / (1.0 + jnp.exp(-gate))) * gain[...]).astype(BF16)
    for i in range(copies):
        sent[i] = u


def chain(arrived, state_high, state_low, base, taps, bias, rate, gain):
    copies, prop, _ = arrived.shape
    inner, heads, width = state_high.shape[0], bias.shape[1], base.shape[1]
    vmem = pl.BlockSpec(memory_space=VMEM)
    return pl.pallas_call(
        chain_kernel,
        in_specs=[vmem] * 8,
        out_specs=[vmem] * 5,
        out_shape=[
            VMEM((copies, prop, inner), BF16),
            VMEM((8, inner), F32),
            VMEM((prop, (width - inner) // 2), F32),
            VMEM((prop, heads), F32),
            VMEM((prop, width), F32),
        ],
        name="chain",
    )(*map(local, (arrived, state_high, state_low, base, taps, bias, rate, gain)))


def states_kernel(
    first, moved, keys, decay, rows, new, new_states, new_v, new_k, new_q, state_s, moved_s, sem_out
):
    prop, heads = decay.shape
    _, _, head_dim, state_dim = state_s.shape
    inner, kwidth = moved.shape[1], keys.shape[1]
    per_group = heads * state_dim // kwidth
    writes = []

    def write(source, slot):
        copy = pltpu.make_async_copy(source, new_states.at[0, slot], sem_out.at[slot])
        copy.start()
        writes.append(copy)

    write(first.at[0], 0)
    at = 0
    for out in (new_v, new_k, new_q):
        width = out.shape[2]
        both = jnp.concatenate([rows[:, at : at + width], new[:, at : at + width]], axis=0)
        out[0] = both.astype(BF16)
        at += width
    for c in range(0, inner, LANES):
        moved_s[c : c + LANES, :] = jnp.transpose(moved[:, c : c + LANES])
    for t in range(prop):
        for h in range(heads):
            g = h // per_group
            before = first[0, h] if t == 0 else state_s[t - 1, h]
            key_row = keys[t : t + 1, g * state_dim : (g + 1) * state_dim]
            column = moved_s[h * head_dim : (h + 1) * head_dim, t : t + 1]
            state_s[t, h] = before * decay[t : t + 1, h : h + 1] + column * key_row
        write(state_s.at[t], t + 1)
    for copy in writes:
        copy.wait()


def next_states(keep, first, moved, keys, decay, rows, new):
    _, heads, head_dim, state_dim = first.shape
    inner, kwidth = moved.shape[1], keys.shape[1]
    count = rows.shape[0] + new.shape[0]
    plain = pl.BlockSpec()
    vmem = pl.BlockSpec(memory_space=VMEM)
    return pl.pallas_call(
        states_kernel,
        in_specs=[vmem] * 6,
        out_specs=[pl.BlockSpec(memory_space=pl.ANY), plain, plain, plain],
        out_shape=[
            jax.ShapeDtypeStruct((1, keep, heads, head_dim, state_dim), F32),
            jax.ShapeDtypeStruct((1, count, inner), BF16),
            jax.ShapeDtypeStruct((1, count, kwidth), BF16),
            jax.ShapeDtypeStruct((1, count, kwidth), BF16),
        ],
        scratch_shapes=[
            VMEM((keep - 1, heads, head_dim, state_dim), F32),
            VMEM((inner, 8), F32),
            pltpu.SemaphoreType.DMA((keep,)),
        ],
        name="states",
    )(*map(local, (first, moved, keys, decay, rows, new)))


def output_kernel(rows, w_out, gain, out):
    features = w_out.shape[0]
    x = rows[...]
    out[:, :features] = lax.dot_general(x, w_out[...], NT, preferred_element_type=F32).astype(BF16)
    wide = x.astype(F32)
    inverse = 1.0 / (gain[...] * gain[...])
    squares = jnp.sum(wide * wide * inverse, axis=1, keepdims=True)
    high, low = halves(squares)
    lane = lane_of((x.shape[0], LANES - features))
    out[:, features:] = jnp.where(lane == 0, high, jnp.where(lane == 1, low, 0.0)).astype(BF16)


def output(rows, w_out, gain):
    vmem = pl.BlockSpec(memory_space=VMEM)
    return pl.pallas_call(
        output_kernel,
        in_specs=[vmem] * 3,
        out_specs=vmem,
        out_shape=VMEM((rows.shape[0], LANES), BF16),
        name="output",
    )(local(rows), local(w_out.T), local(gain))


def combine_kernel(mine, other, out):
    seqs, prop, features = out.shape
    a, b = mine[...].astype(F32), other[...].astype(F32)
    squares_a = a[:, features : features + 1] + a[:, features + 1 : features + 2]
    squares_b = b[:, features : features + 1] + b[:, features + 1 : features + 2]
    scale = lax.rsqrt((squares_a + squares_b) / WIDTH + EPS)
    mixed = (a[:, :features] + b[:, :features]) * scale
    for i in range(seqs):
        out[i] = mixed[prop * i : prop * (i + 1)].astype(BF16)


def combine(mine, other, seqs, features):
    vmem = pl.BlockSpec(memory_space=VMEM)
    return pl.pallas_call(
        combine_kernel,
        in_specs=[vmem, vmem],
        out_shape=jax.ShapeDtypeStruct((seqs, mine.shape[0] // seqs, features), BF16),
        name="combine",
    )(local(mine), local(other))


def per_device(
    tokens,
    in_gain,
    w_gate,
    w_value,
    w_key,
    w_query,
    w_step,
    conv_value,
    conv_key,
    conv_query,
    step_bias,
    decay_log,
    out_gain,
    w_out,
    past_value,
    past_key,
    past_query,
    past_states,
    accepted,
):
    group_seqs, proposals, features = tokens.shape
    partial = project(tokens, in_gain, (w_gate, w_value, w_key, w_query, w_step))
    arrived = lax.all_to_all(partial, "kv", 0, 0, tiled=True)
    first, high, low, rows, base, taps, bias, rate, gain = prepare(
        accepted,
        past_states,
        (past_value, past_key, past_query),
        (conv_value, conv_key, conv_query),
        step_bias,
        decay_log,
        out_gain,
    )
    sent, moved, keys, decay, new = chain(arrived, high, low, base, taps, bias, rate, gain)
    gathered = lax.all_to_all(sent, "kv", 0, 0, tiled=True)
    saved = next_states(past_states.shape[1], first, moved, keys, decay, rows, new)
    mine = output(gathered.reshape(group_seqs * proposals, -1), w_out, gain)
    swap = [(i, 1 - i) for i in range(2)]
    mixed = combine(mine, lax.ppermute(mine, "tp", swap), group_seqs, features)
    return (mixed, *saved)


def solution(mesh):
    placed = (
        P("dp", None, "kv"),
        P("kv"),
        P("kv", "tp"),
        P("kv", "tp"),
        P("kv", "tp"),
        P("kv", "tp"),
        P("kv", "tp"),
        P(None, "tp"),
        P(None, "tp"),
        P(None, "tp"),
        P("tp"),
        P("tp"),
        P("tp"),
        P("tp", "kv"),
        P(("dp", "kv"), None, "tp"),
        P(("dp", "kv"), None, "tp"),
        P(("dp", "kv"), None, "tp"),
        P(("dp", "kv"), None, "tp", None, None),
        P(("dp", "kv")),
    )
    return jax.shard_map(
        per_device,
        mesh=mesh,
        in_specs=placed,
        out_specs=(
            P("dp", None, "kv"),
            P(("dp", "kv"), None, "tp", None, None),
            P(("dp", "kv"), None, "tp"),
            P(("dp", "kv"), None, "tp"),
            P(("dp", "kv"), None, "tp"),
        ),
        check_vma=False,
    )
```

```python
import functools

import jax
import jax.numpy as jnp
from jax import lax
from jax.experimental import pallas as pl
from jax.experimental.pallas import tpu as pltpu
from jax.sharding import PartitionSpec as P

D = 2048
CONV = 4
WIDTH = 2048
EPS = 1e-05
KV = ("kz", "ky")
NEAR = 4

F32 = jnp.float32
BF16 = jnp.bfloat16
LANES = 128
VMEM = pltpu.VMEM
NT = (((1,), (1,)), ((), ()))


def local(x):
    return pltpu.with_memory_space_constraint(x, VMEM)


def lane_of(shape):
    return lax.broadcasted_iota(jnp.int32, shape, 1)


def halves(x):
    high = x.astype(BF16).astype(F32)
    return high, x - high


def project_kernel(tok, gain, wg, wv, wk, wq, ws, out, x_s, ws_s):
    seqs, prop, _ = tok.shape
    near, block, _ = out.shape
    far = seqs // near
    for i in range(seqs):
        at = prop * ((i % near) * far + i // near)
        x_s[at : at + prop, :] = tok[i].astype(F32)
    ws_s[...] = jnp.zeros(ws_s.shape, BF16)
    ws_s[: ws.shape[0], :] = ws[...]
    x = x_s[...]
    squares = jnp.sum(x * x, axis=1, keepdims=True)
    normed = (x * gain[...]).astype(BF16)

    def put(at, product):
        width = product.shape[1]
        rounded = product.astype(BF16)
        for j in range(near):
            out[j, :, at : at + width] = rounded[block * j : block * (j + 1)]

    at = 0
    for w in (wg, wv, wk, wq):
        for c in range(0, w.shape[1], 256):
            put(at, jnp.dot(normed, w[:, c : c + 256], preferred_element_type=F32))
            at += 256
    heads = ws.shape[0]
    extra = lax.dot_general(normed, ws_s[...], NT, preferred_element_type=F32)
    put(at, with_squares(extra, squares, heads))


def with_squares(extra, squares, at):
    high, low = halves(squares)
    lane = lane_of(extra.shape)
    return jnp.where(lane == at, high, jnp.where(lane == at + 1, low, extra))


def project(tokens, gain, weights, near):
    seqs, prop, feat = tokens.shape
    columns = sum(w.shape[1] for w in weights[:4]) + LANES
    return pl.pallas_call(
        project_kernel,
        out_specs=pl.BlockSpec(memory_space=VMEM),
        out_shape=VMEM((near, seqs // near * prop, columns), BF16),
        scratch_shapes=[VMEM((seqs * prop, feat), F32), VMEM((LANES, feat), BF16)],
        name="project",
    )(tokens, gain.reshape(1, feat), *weights[:4], weights[4].T)


def fold_kernel(heads, arrived, out):
    near, _, columns = arrived.shape
    far, prop, _ = out.shape
    for at in range(0, columns, LANES):
        total = arrived[0, :, at : at + LANES].astype(F32)
        for j in range(1, near):
            total = total + arrived[j, :, at : at + LANES].astype(F32)
        if at == columns - LANES:
            squares = total[:, heads : heads + 1] + total[:, heads + 1 : heads + 2]
            total = with_squares(total, squares, heads)
        for k in range(far):
            out[k, :, at : at + LANES] = total[prop * k : prop * (k + 1)].astype(BF16)


def fold(arrived, far, heads):
    _, rows, columns = arrived.shape
    vmem = pl.BlockSpec(memory_space=VMEM)
    return pl.pallas_call(
        functools.partial(fold_kernel, heads),
        in_specs=[vmem],
        out_specs=vmem,
        out_shape=VMEM((far, rows // far, columns), BF16),
        name="fold",
    )(local(arrived))


def prepare_kernel(
    accepted,
    states,
    past_v,
    past_k,
    past_q,
    taps_v,
    taps_k,
    taps_q,
    bias,
    log_rate,
    out_gain,
    state,
    state_high,
    state_low,
    rows,
    base,
    taps,
    bias_out,
    rate,
    gain,
    sem,
):
    offset = accepted[0]
    fetch = pltpu.make_async_copy(states.at[0, pl.ds(offset, 1)], state, sem)
    fetch.start()
    span, prop = rows.shape[0], base.shape[0]
    at = 0
    for past, tap in ((past_v, taps_v), (past_k, taps_k), (past_q, taps_q)):
        width = past.shape[2]
        history = past[0].astype(F32)
        picked = history[0:span]
        for j in range(1, history.shape[0] - span + 1):
            picked = jnp.where(offset == j, history[j : j + span], picked)
        weight = tap[...].astype(F32)
        rows[:, at : at + width] = picked
        taps[:, at : at + width] = weight
        for t in range(prop):
            part = jnp.zeros((1, width), F32)
            for i in range(CONV):
                if t + i < span:
                    part = part + picked[t + i : t + i + 1] * weight[i : i + 1]
            base[t : t + 1, at : at + width] = part
        at += width
    bias_out[...] = bias[...]
    rate[...] = -jnp.exp(log_rate[...])
    gain[...] = out_gain[...]
    fetch.wait()
    for h in range(state.shape[1]):
        at = slice(h * state.shape[2], (h + 1) * state.shape[2])
        high = state[0, h].astype(BF16)
        state_high[at] = high
        state_low[at] = (state[0, h] - high.astype(F32)).astype(BF16)


def prepare(accepted, states, pasts, taps, bias, log_rate, out_gain):
    _, _, heads, head_dim, state_dim = states.shape
    inner = heads * head_dim
    width = sum(p.shape[2] for p in pasts)
    prop = pasts[0].shape[1] - (CONV - 1)
    plain, vmem = pl.BlockSpec(), pl.BlockSpec(memory_space=VMEM)
    return pl.pallas_call(
        prepare_kernel,
        in_specs=[pl.BlockSpec(memory_space=pltpu.SMEM), pl.BlockSpec(memory_space=pl.ANY), *[plain] * 9],
        out_specs=[vmem] * 9,
        out_shape=[
            VMEM((1, heads, head_dim, state_dim), F32),
            VMEM((inner, state_dim), BF16),
            VMEM((inner, state_dim), BF16),
            VMEM((CONV - 1, width), F32),
            VMEM((prop, width), F32),
            VMEM((CONV, width), F32),
            VMEM((1, heads), F32),
            VMEM((1, heads), F32),
            VMEM((1, inner), F32),
        ],
        scratch_shapes=[pltpu.SemaphoreType.DMA(())],
        name="prepare",
    )(
        accepted,
        states,
        *pasts,
        *taps,
        bias.reshape(1, heads),
        log_rate.reshape(1, heads),
        out_gain.reshape(1, inner),
    )


def chain_kernel(
    arrived, state_high, state_low, base, taps, bias, rate, gain, sent, moved_out, key_out, decay_out, new_out
):
    copies, prop, _ = arrived.shape
    inner, state_dim = state_high.shape
    heads = bias.shape[1]
    head_dim = inner // heads
    width = base.shape[1]
    kwidth = (width - inner) // 2
    groups = kwidth // state_dim
    per_group = inner // groups

    total = arrived[0].astype(F32)
    for i in range(1, copies):
        total = total + arrived[i].astype(F32)
    at_step = inner + width
    squares = total[:, at_step + heads : at_step + heads + 1] + total[:, at_step + heads + 1 : at_step + heads + 2]
    rscale = lax.rsqrt(squares / D + EPS)

    def scaled(start, stop):
        return (total[:, start:stop] * rscale).astype(BF16).astype(F32)

    new = scaled(inner, at_step)
    new_out[...] = new
    filtered = base[...] + new * taps[CONV - 1 : CONV]
    for i in range(1, CONV):
        later = jnp.concatenate([jnp.zeros((i, width), F32), new[: prop - i]], axis=0)
        filtered = filtered + later * taps[CONV - 1 - i : CONV - i]
    convolved = filtered / (1.0 + jnp.exp(-filtered))
    conv_v, conv_k, conv_q = convolved[:, :inner], convolved[:, inner : inner + kwidth], convolved[:, inner + kwidth :]

    raw = total[:, at_step : at_step + heads] * rscale + bias[...]
    steps = jnp.maximum(raw, 0.0) + jnp.log1p(jnp.exp(-jnp.abs(raw)))
    decay = jnp.exp(steps * rate[...])
    first_half = lane_of((prop, 2 * head_dim)) < head_dim

    def spread(x):
        return jnp.concatenate(
            [jnp.where(first_half, x[:, h : h + 1], x[:, h + 1 : h + 2]) for h in range(0, heads, 2)], axis=1
        )

    moved = spread(steps) * conv_v
    shrink = spread(decay)
    moved_out[0:prop, :] = moved
    moved_out[prop:, :] = jnp.zeros((moved_out.shape[0] - prop, inner), F32)
    key_out[...] = conv_k
    decay_out[...] = decay

    q_high, q_low = halves(conv_q)
    q_both = jnp.concatenate([q_high, q_low], axis=0).astype(BF16)
    row = lax.broadcasted_iota(jnp.int32, (prop, per_group), 0)
    ys = []
    for g in range(groups):
        cols = slice(g * per_group, (g + 1) * per_group)
        part = slice(g * state_dim, (g + 1) * state_dim)
        main = lax.dot_general(q_both[:, part], state_high[cols], NT, preferred_element_type=F32)
        rest = lax.dot_general(q_both[:prop, part], state_low[cols], NT, preferred_element_type=F32)
        carried = main[:prop] + main[prop:] + rest
        y = jnp.zeros((prop, per_group), F32)
        for t in range(prop):
            match = jnp.sum(conv_q[:, part] * conv_k[t : t + 1, part], axis=1, keepdims=True)
            carried = carried * shrink[t : t + 1, cols] + moved[t : t + 1, cols] * match
            y = jnp.where(row == t, carried, y)
        ys.append(y)
    y = jnp.concatenate(ys, axis=1)
    gate = scaled(0, inner)
    u = (y * (gate / (1.0 + jnp.exp(-gate))) * gain[...]).astype(BF16)
    for i in range(sent.shape[0]):
        sent[i] = u


def chain(copies, arrived, state_high, state_low, base, taps, bias, rate, gain):
    prop = arrived.shape[1]
    inner, heads, width = state_high.shape[0], bias.shape[1], base.shape[1]
    vmem = pl.BlockSpec(memory_space=VMEM)
    return pl.pallas_call(
        chain_kernel,
        in_specs=[vmem] * 8,
        out_specs=[vmem] * 5,
        out_shape=[
            VMEM((copies, prop, inner), BF16),
            VMEM((8, inner), F32),
            VMEM((prop, (width - inner) // 2), F32),
            VMEM((prop, heads), F32),
            VMEM((prop, width), F32),
        ],
        name="chain",
    )(*map(local, (arrived, state_high, state_low, base, taps, bias, rate, gain)))


def states_kernel(
    first, moved, keys, decay, rows, new, new_states, new_v, new_k, new_q, state_s, moved_s, sem_out
):
    prop, heads = decay.shape
    _, _, head_dim, state_dim = state_s.shape
    inner, kwidth = moved.shape[1], keys.shape[1]
    per_group = heads * state_dim // kwidth
    writes = []

    def write(source, slot):
        copy = pltpu.make_async_copy(source, new_states.at[0, slot], sem_out.at[slot])
        copy.start()
        writes.append(copy)

    write(first.at[0], 0)
    at = 0
    for out in (new_v, new_k, new_q):
        width = out.shape[2]
        both = jnp.concatenate([rows[:, at : at + width], new[:, at : at + width]], axis=0)
        out[0] = both.astype(BF16)
        at += width
    for c in range(0, inner, LANES):
        moved_s[c : c + LANES, :] = jnp.transpose(moved[:, c : c + LANES])
    for t in range(prop):
        for h in range(heads):
            g = h // per_group
            before = first[0, h] if t == 0 else state_s[t - 1, h]
            key_row = keys[t : t + 1, g * state_dim : (g + 1) * state_dim]
            column = moved_s[h * head_dim : (h + 1) * head_dim, t : t + 1]
            state_s[t, h] = before * decay[t : t + 1, h : h + 1] + column * key_row
        write(state_s.at[t], t + 1)
    for copy in writes:
        copy.wait()


def next_states(keep, first, moved, keys, decay, rows, new):
    _, heads, head_dim, state_dim = first.shape
    inner, kwidth = moved.shape[1], keys.shape[1]
    count = rows.shape[0] + new.shape[0]
    plain = pl.BlockSpec()
    vmem = pl.BlockSpec(memory_space=VMEM)
    return pl.pallas_call(
        states_kernel,
        in_specs=[vmem] * 6,
        out_specs=[pl.BlockSpec(memory_space=pl.ANY), plain, plain, plain],
        out_shape=[
            jax.ShapeDtypeStruct((1, keep, heads, head_dim, state_dim), F32),
            jax.ShapeDtypeStruct((1, count, inner), BF16),
            jax.ShapeDtypeStruct((1, count, kwidth), BF16),
            jax.ShapeDtypeStruct((1, count, kwidth), BF16),
        ],
        scratch_shapes=[
            VMEM((keep - 1, heads, head_dim, state_dim), F32),
            VMEM((inner, 8), F32),
            pltpu.SemaphoreType.DMA((keep,)),
        ],
        name="states",
    )(*map(local, (first, moved, keys, decay, rows, new)))


def output_kernel(rows, w_out, gain, out):
    features = w_out.shape[0]
    x = rows[...]
    out[:, :features] = lax.dot_general(x, w_out[...], NT, preferred_element_type=F32).astype(BF16)
    wide = x.astype(F32)
    inverse = 1.0 / (gain[...] * gain[...])
    squares = jnp.sum(wide * wide * inverse, axis=1, keepdims=True)
    high, low = halves(squares)
    lane = lane_of((x.shape[0], LANES - features))
    out[:, features:] = jnp.where(lane == 0, high, jnp.where(lane == 1, low, 0.0)).astype(BF16)


def output(rows, w_out, gain):
    vmem = pl.BlockSpec(memory_space=VMEM)
    return pl.pallas_call(
        output_kernel,
        in_specs=[vmem] * 3,
        out_specs=vmem,
        out_shape=VMEM((rows.shape[0], LANES), BF16),
        name="output",
    )(local(rows), local(w_out.T), local(gain))


def combine_kernel(mine, other, out):
    seqs, prop, features = out.shape
    a, b = mine[...].astype(F32), other[...].astype(F32)
    squares_a = a[:, features : features + 1] + a[:, features + 1 : features + 2]
    squares_b = b[:, features : features + 1] + b[:, features + 1 : features + 2]
    scale = lax.rsqrt((squares_a + squares_b) / WIDTH + EPS)
    mixed = (a[:, :features] + b[:, :features]) * scale
    for i in range(seqs):
        out[i] = mixed[prop * i : prop * (i + 1)].astype(BF16)


def combine(mine, other, seqs, features):
    vmem = pl.BlockSpec(memory_space=VMEM)
    return pl.pallas_call(
        combine_kernel,
        in_specs=[vmem, vmem],
        out_shape=jax.ShapeDtypeStruct((seqs, mine.shape[0] // seqs, features), BF16),
        name="combine",
    )(local(mine), local(other))


def per_device(
    tokens,
    in_gain,
    w_gate,
    w_value,
    w_key,
    w_query,
    w_step,
    conv_value,
    conv_key,
    conv_query,
    step_bias,
    decay_log,
    out_gain,
    w_out,
    past_value,
    past_key,
    past_query,
    past_states,
    accepted,
):
    group_seqs, proposals, features = tokens.shape
    weights = (w_gate, w_value, w_key, w_query, w_step)
    partial = project(tokens, in_gain, weights, lax.axis_size("ky"))
    nearby = lax.all_to_all(partial, "ky", 0, 0, tiled=True)
    first, high, low, rows, base, taps, bias, rate, gain = prepare(
        accepted,
        past_states,
        (past_value, past_key, past_query),
        (conv_value, conv_key, conv_query),
        step_bias,
        decay_log,
        out_gain,
    )
    partial = fold(nearby, lax.axis_size("kz"), w_step.shape[1])
    arrived = lax.all_to_all(partial, "kz", 0, 0, tiled=True)
    sent, moved, keys, decay, new = chain(group_seqs, arrived, high, low, base, taps, bias, rate, gain)
    gathered = lax.all_to_all(sent, KV, 0, 0, tiled=True)
    saved = next_states(past_states.shape[1], first, moved, keys, decay, rows, new)
    mine = output(gathered.reshape(group_seqs * proposals, -1), w_out, gain)
    swap = [(i, 1 - i) for i in range(2)]
    mixed = combine(mine, lax.ppermute(mine, "tp", swap), group_seqs, features)
    return (mixed, *saved)


def solution(mesh):
    dp, kv, tp = mesh.devices.shape
    near = NEAR if kv % NEAR == 0 else 1
    split = jax.sharding.Mesh(mesh.devices.reshape(dp, kv // near, near, tp), ("dp", *KV, "tp"))
    placed = (
        P("dp", None, KV),
        P(KV),
        P(KV, "tp"),
        P(KV, "tp"),
        P(KV, "tp"),
        P(KV, "tp"),
        P(KV, "tp"),
        P(None, "tp"),
        P(None, "tp"),
        P(None, "tp"),
        P("tp"),
        P("tp"),
        P("tp"),
        P("tp", KV),
        P(("dp", *KV), None, "tp"),
        P(("dp", *KV), None, "tp"),
        P(("dp", *KV), None, "tp"),
        P(("dp", *KV), None, "tp", None, None),
        P(("dp", *KV)),
    )
    return jax.shard_map(
        per_device,
        mesh=split,
        in_specs=placed,
        out_specs=(
            P("dp", None, KV),
            P(("dp", *KV), None, "tp", None, None),
            P(("dp", *KV), None, "tp"),
            P(("dp", *KV), None, "tp"),
            P(("dp", *KV), None, "tp"),
        ),
        check_vma=False,
    )
```

```python
import functools

import jax
import jax.numpy as jnp
from jax import lax
from jax.experimental import pallas as pl
from jax.experimental.pallas import tpu as pltpu
from jax.sharding import PartitionSpec as P

D = 2048
CONV = 4
WIDTH = 2048
EPS = 1e-05
KV = ("kz", "ky")
NEAR = 4

F32 = jnp.float32
BF16 = jnp.bfloat16
LANES = 128
VMEM = pltpu.VMEM
NT = (((1,), (1,)), ((), ()))


def local(x):
    return pltpu.with_memory_space_constraint(x, VMEM)


def lane_of(shape):
    return lax.broadcasted_iota(jnp.int32, shape, 1)


def halves(x):
    high = x.astype(BF16).astype(F32)
    return high, x - high


def with_squares(extra, squares, at):
    high, low = halves(squares)
    lane = lane_of(extra.shape)
    return jnp.where(lane == at, high, jnp.where(lane == at + 1, low, extra))


def first_kernel(*refs):
    sources, results, scratch = refs[:18], refs[18:28], refs[28:]
    accepted, states, *plain = sources
    out, state, state_high, state_low, rows, base, taps, bias, rate, gain = results
    accepted_s, tok, in_gain, wg, wv, wk, wq, ws, pv, pk, pq, tv, tk, tq, log_rate, x_s, ws_s, sems = scratch

    def copy(source, target, slot):
        moving = pltpu.make_async_copy(source, target, sems.at[slot])
        moving.start()
        return moving

    offset_copy = copy(accepted, accepted_s, 0)
    targets = (tok, in_gain, wg, wv, wk, wq, ws, pv, pk, pq, tv, tk, tq, bias, log_rate, gain)
    copies = [copy(source, target, 2 + n) for n, (source, target) in enumerate(zip(plain, targets))]
    ws_s[...] = jnp.zeros(ws_s.shape, BF16)
    offset_copy.wait()
    offset = accepted_s[0, 0]
    fetch = copy(states.at[0, pl.ds(offset, 1)], state, 1)

    copies[0].wait()
    copies[1].wait()
    seqs, prop, _ = tok.shape
    near, block, _ = out.shape
    far = seqs // near
    for i in range(seqs):
        at = prop * ((i % near) * far + i // near)
        x_s[at : at + prop, :] = tok[i].astype(F32)
    x = x_s[...]
    squares = jnp.sum(x * x, axis=1, keepdims=True)
    normed = (x * in_gain[...]).astype(BF16)

    def put(at, product):
        width = product.shape[1]
        rounded = product.astype(BF16)
        for j in range(near):
            out[j, :, at : at + width] = rounded[block * j : block * (j + 1)]

    at = 0
    for n, w in enumerate((wg, wv, wk, wq)):
        copies[2 + n].wait()
        for c in range(0, w.shape[1], 256):
            put(at, jnp.dot(normed, w[:, c : c + 256], preferred_element_type=F32))
            at += 256
    copies[6].wait()
    heads = ws.shape[0]
    ws_s[:heads, :] = ws[...]
    extra = lax.dot_general(normed, ws_s[...], NT, preferred_element_type=F32)
    put(at, with_squares(extra, squares, heads))

    for n in range(7, 16):
        copies[n].wait()
    rate[...] = -jnp.exp(log_rate[...])
    span = rows.shape[0]
    at = 0
    for past, tap in ((pv, tv), (pk, tk), (pq, tq)):
        width = past.shape[2]
        history = past[0].astype(F32)
        picked = history[0:span]
        for j in range(1, history.shape[0] - span + 1):
            picked = jnp.where(offset == j, history[j : j + span], picked)
        weight = tap[...].astype(F32)
        rows[:, at : at + width] = picked
        taps[:, at : at + width] = weight
        for t in range(prop):
            part = jnp.zeros((1, width), F32)
            for i in range(CONV):
                if t + i < span:
                    part = part + picked[t + i : t + i + 1] * weight[i : i + 1]
            base[t : t + 1, at : at + width] = part
        at += width

    fetch.wait()
    for h in range(state.shape[1]):
        at = slice(h * state.shape[2], (h + 1) * state.shape[2])
        high = state[0, h].astype(BF16)
        state_high[at] = high
        state_low[at] = (state[0, h] - high.astype(F32)).astype(BF16)


def first(near, accepted, states, tokens, in_gain, weights, pasts, taps, bias, log_rate, out_gain):
    seqs, prop, feat = tokens.shape
    _, _, heads, head_dim, state_dim = states.shape
    inner = heads * head_dim
    width = sum(p.shape[2] for p in pasts)
    columns = sum(w.shape[1] for w in weights[:4]) + LANES
    row = (tokens, in_gain.reshape(1, feat), *weights[:4], weights[4].T, *pasts, *taps)
    row = (*row, bias.reshape(1, heads), log_rate.reshape(1, heads), out_gain.reshape(1, inner))
    landing = [VMEM(x.shape, x.dtype) for x in row]
    return pl.pallas_call(
        first_kernel,
        in_specs=[pl.BlockSpec(memory_space=pltpu.HBM)] * 18,
        out_specs=[pl.BlockSpec(memory_space=VMEM)] * 10,
        out_shape=[
            VMEM((near, seqs // near * prop, columns), BF16),
            VMEM((1, heads, head_dim, state_dim), F32),
            VMEM((inner, state_dim), BF16),
            VMEM((inner, state_dim), BF16),
            VMEM((CONV - 1, width), F32),
            VMEM((prop, width), F32),
            VMEM((CONV, width), F32),
            VMEM((1, heads), F32),
            VMEM((1, heads), F32),
            VMEM((1, inner), F32),
        ],
        scratch_shapes=[
            pltpu.SMEM((1, 1), jnp.int32),
            *landing[:13],
            landing[14],
            VMEM((seqs * prop, feat), F32),
            VMEM((LANES, feat), BF16),
            pltpu.SemaphoreType.DMA((18,)),
        ],
        name="first",
    )(accepted.reshape(1, 1), states, *row)


def fold_kernel(heads, arrived, out):
    near, _, columns = arrived.shape
    far, prop, _ = out.shape
    for at in range(0, columns, LANES):
        total = arrived[0, :, at : at + LANES].astype(F32)
        for j in range(1, near):
            total = total + arrived[j, :, at : at + LANES].astype(F32)
        if at == columns - LANES:
            squares = total[:, heads : heads + 1] + total[:, heads + 1 : heads + 2]
            total = with_squares(total, squares, heads)
        for k in range(far):
            out[k, :, at : at + LANES] = total[prop * k : prop * (k + 1)].astype(BF16)


def fold(arrived, far, heads):
    _, rows, columns = arrived.shape
    vmem = pl.BlockSpec(memory_space=VMEM)
    return pl.pallas_call(
        functools.partial(fold_kernel, heads),
        in_specs=[vmem],
        out_specs=vmem,
        out_shape=VMEM((far, rows // far, columns), BF16),
        name="fold",
    )(local(arrived))


def chain_kernel(
    arrived, state_high, state_low, base, taps, bias, rate, gain, sent, moved_out, key_out, decay_out, new_out
):
    copies, prop, _ = arrived.shape
    inner, state_dim = state_high.shape
    heads = bias.shape[1]
    head_dim = inner // heads
    width = base.shape[1]
    kwidth = (width - inner) // 2
    groups = kwidth // state_dim
    per_group = inner // groups

    total = arrived[0].astype(F32)
    for i in range(1, copies):
        total = total + arrived[i].astype(F32)
    at_step = inner + width
    squares = total[:, at_step + heads : at_step + heads + 1] + total[:, at_step + heads + 1 : at_step + heads + 2]
    rscale = lax.rsqrt(squares / D + EPS)

    def scaled(start, stop):
        return (total[:, start:stop] * rscale).astype(BF16).astype(F32)

    new = scaled(inner, at_step)
    new_out[...] = new
    filtered = base[...] + new * taps[CONV - 1 : CONV]
    for i in range(1, CONV):
        later = jnp.concatenate([jnp.zeros((i, width), F32), new[: prop - i]], axis=0)
        filtered = filtered + later * taps[CONV - 1 - i : CONV - i]
    convolved = filtered / (1.0 + jnp.exp(-filtered))
    conv_v, conv_k, conv_q = convolved[:, :inner], convolved[:, inner : inner + kwidth], convolved[:, inner + kwidth :]

    raw = total[:, at_step : at_step + heads] * rscale + bias[...]
    steps = jnp.maximum(raw, 0.0) + jnp.log1p(jnp.exp(-jnp.abs(raw)))
    decay = jnp.exp(steps * rate[...])
    first_half = lane_of((prop, 2 * head_dim)) < head_dim

    def spread(x):
        return jnp.concatenate(
            [jnp.where(first_half, x[:, h : h + 1], x[:, h + 1 : h + 2]) for h in range(0, heads, 2)], axis=1
        )

    moved = spread(steps) * conv_v
    shrink = spread(decay)
    moved_out[0:prop, :] = moved
    moved_out[prop:, :] = jnp.zeros((moved_out.shape[0] - prop, inner), F32)
    key_out[...] = conv_k
    decay_out[...] = decay

    q_high, q_low = halves(conv_q)
    q_both = jnp.concatenate([q_high, q_low], axis=0).astype(BF16)
    row = lax.broadcasted_iota(jnp.int32, (prop, per_group), 0)
    ys = []
    for g in range(groups):
        cols = slice(g * per_group, (g + 1) * per_group)
        part = slice(g * state_dim, (g + 1) * state_dim)
        main = lax.dot_general(q_both[:, part], state_high[cols], NT, preferred_element_type=F32)
        rest = lax.dot_general(q_both[:prop, part], state_low[cols], NT, preferred_element_type=F32)
        carried = main[:prop] + main[prop:] + rest
        y = jnp.zeros((prop, per_group), F32)
        for t in range(prop):
            match = jnp.sum(conv_q[:, part] * conv_k[t : t + 1, part], axis=1, keepdims=True)
            carried = carried * shrink[t : t + 1, cols] + moved[t : t + 1, cols] * match
            y = jnp.where(row == t, carried, y)
        ys.append(y)
    y = jnp.concatenate(ys, axis=1)
    gate = scaled(0, inner)
    u = (y * (gate / (1.0 + jnp.exp(-gate))) * gain[...]).astype(BF16)
    for i in range(sent.shape[0]):
        sent[i] = u


def chain(copies, arrived, state_high, state_low, base, taps, bias, rate, gain):
    prop = arrived.shape[1]
    inner, heads, width = state_high.shape[0], bias.shape[1], base.shape[1]
    vmem = pl.BlockSpec(memory_space=VMEM)
    return pl.pallas_call(
        chain_kernel,
        in_specs=[vmem] * 8,
        out_specs=[vmem] * 5,
        out_shape=[
            VMEM((copies, prop, inner), BF16),
            VMEM((8, inner), F32),
            VMEM((prop, (width - inner) // 2), F32),
            VMEM((prop, heads), F32),
            VMEM((prop, width), F32),
        ],
        name="chain",
    )(*map(local, (arrived, state_high, state_low, base, taps, bias, rate, gain)))


def states_kernel(
    first, moved, keys, decay, rows, new, new_states, new_v, new_k, new_q, state_s, moved_s, sem_out
):
    prop, heads = decay.shape
    _, _, head_dim, state_dim = state_s.shape
    inner, kwidth = moved.shape[1], keys.shape[1]
    per_group = heads * state_dim // kwidth
    writes = []

    def write(source, slot):
        copy = pltpu.make_async_copy(source, new_states.at[0, slot], sem_out.at[slot])
        copy.start()
        writes.append(copy)

    write(first.at[0], 0)
    at = 0
    for out in (new_v, new_k, new_q):
        width = out.shape[2]
        both = jnp.concatenate([rows[:, at : at + width], new[:, at : at + width]], axis=0)
        out[0] = both.astype(BF16)
        at += width
    for c in range(0, inner, LANES):
        moved_s[c : c + LANES, :] = jnp.transpose(moved[:, c : c + LANES])
    for t in range(prop):
        for h in range(heads):
            g = h // per_group
            before = first[0, h] if t == 0 else state_s[t - 1, h]
            key_row = keys[t : t + 1, g * state_dim : (g + 1) * state_dim]
            column = moved_s[h * head_dim : (h + 1) * head_dim, t : t + 1]
            state_s[t, h] = before * decay[t : t + 1, h : h + 1] + column * key_row
        write(state_s.at[t], t + 1)
    for copy in writes:
        copy.wait()


def next_states(keep, first, moved, keys, decay, rows, new):
    _, heads, head_dim, state_dim = first.shape
    inner, kwidth = moved.shape[1], keys.shape[1]
    count = rows.shape[0] + new.shape[0]
    plain = pl.BlockSpec()
    vmem = pl.BlockSpec(memory_space=VMEM)
    return pl.pallas_call(
        states_kernel,
        in_specs=[vmem] * 6,
        out_specs=[pl.BlockSpec(memory_space=pl.ANY), plain, plain, plain],
        out_shape=[
            jax.ShapeDtypeStruct((1, keep, heads, head_dim, state_dim), F32),
            jax.ShapeDtypeStruct((1, count, inner), BF16),
            jax.ShapeDtypeStruct((1, count, kwidth), BF16),
            jax.ShapeDtypeStruct((1, count, kwidth), BF16),
        ],
        scratch_shapes=[
            VMEM((keep - 1, heads, head_dim, state_dim), F32),
            VMEM((inner, 8), F32),
            pltpu.SemaphoreType.DMA((keep,)),
        ],
        name="states",
    )(*map(local, (first, moved, keys, decay, rows, new)))


def output_kernel(rows, w_out, gain, out):
    features = w_out.shape[0]
    x = rows[...]
    out[:, :features] = lax.dot_general(x, w_out[...], NT, preferred_element_type=F32).astype(BF16)
    wide = x.astype(F32)
    inverse = 1.0 / (gain[...] * gain[...])
    squares = jnp.sum(wide * wide * inverse, axis=1, keepdims=True)
    high, low = halves(squares)
    lane = lane_of((x.shape[0], LANES - features))
    out[:, features:] = jnp.where(lane == 0, high, jnp.where(lane == 1, low, 0.0)).astype(BF16)


def output(rows, w_out, gain):
    vmem = pl.BlockSpec(memory_space=VMEM)
    return pl.pallas_call(
        output_kernel,
        in_specs=[vmem] * 3,
        out_specs=vmem,
        out_shape=VMEM((rows.shape[0], LANES), BF16),
        name="output",
    )(local(rows), local(w_out.T), local(gain))


def combine_kernel(mine, other, out):
    seqs, prop, features = out.shape
    a, b = mine[...].astype(F32), other[...].astype(F32)
    squares_a = a[:, features : features + 1] + a[:, features + 1 : features + 2]
    squares_b = b[:, features : features + 1] + b[:, features + 1 : features + 2]
    scale = lax.rsqrt((squares_a + squares_b) / WIDTH + EPS)
    mixed = (a[:, :features] + b[:, :features]) * scale
    for i in range(seqs):
        out[i] = mixed[prop * i : prop * (i + 1)].astype(BF16)


def combine(mine, other, seqs, features):
    vmem = pl.BlockSpec(memory_space=VMEM)
    return pl.pallas_call(
        combine_kernel,
        in_specs=[vmem, vmem],
        out_shape=jax.ShapeDtypeStruct((seqs, mine.shape[0] // seqs, features), BF16),
        name="combine",
    )(local(mine), local(other))


def per_device(
    tokens,
    in_gain,
    w_gate,
    w_value,
    w_key,
    w_query,
    w_step,
    conv_value,
    conv_key,
    conv_query,
    step_bias,
    decay_log,
    out_gain,
    w_out,
    past_value,
    past_key,
    past_query,
    past_states,
    accepted,
):
    group_seqs, proposals, features = tokens.shape
    partial, state, high, low, rows, base, taps, bias, rate, gain = first(
        lax.axis_size("ky"),
        accepted,
        past_states,
        tokens,
        in_gain,
        (w_gate, w_value, w_key, w_query, w_step),
        (past_value, past_key, past_query),
        (conv_value, conv_key, conv_query),
        step_bias,
        decay_log,
        out_gain,
    )
    nearby = lax.all_to_all(partial, "ky", 0, 0, tiled=True)
    partial = fold(nearby, lax.axis_size("kz"), w_step.shape[1])
    arrived = lax.all_to_all(partial, "kz", 0, 0, tiled=True)
    sent, moved, keys, decay, new = chain(group_seqs, arrived, high, low, base, taps, bias, rate, gain)
    gathered = lax.all_to_all(sent, KV, 0, 0, tiled=True)
    saved = next_states(past_states.shape[1], state, moved, keys, decay, rows, new)
    mine = output(gathered.reshape(group_seqs * proposals, -1), w_out, gain)
    swap = [(i, 1 - i) for i in range(2)]
    mixed = combine(mine, lax.ppermute(mine, "tp", swap), group_seqs, features)
    return (mixed, *saved)


def solution(mesh):
    dp, kv, tp = mesh.devices.shape
    near = NEAR if kv % NEAR == 0 else 1
    split = jax.sharding.Mesh(mesh.devices.reshape(dp, kv // near, near, tp), ("dp", *KV, "tp"))
    placed = (
        P("dp", None, KV),
        P(KV),
        P(KV, "tp"),
        P(KV, "tp"),
        P(KV, "tp"),
        P(KV, "tp"),
        P(KV, "tp"),
        P(None, "tp"),
        P(None, "tp"),
        P(None, "tp"),
        P("tp"),
        P("tp"),
        P("tp"),
        P("tp", KV),
        P(("dp", *KV), None, "tp"),
        P(("dp", *KV), None, "tp"),
        P(("dp", *KV), None, "tp"),
        P(("dp", *KV), None, "tp", None, None),
        P(("dp", *KV)),
    )
    return jax.shard_map(
        per_device,
        mesh=split,
        in_specs=placed,
        out_specs=(
            P("dp", None, KV),
            P(("dp", *KV), None, "tp", None, None),
            P(("dp", *KV), None, "tp"),
            P(("dp", *KV), None, "tp"),
            P(("dp", *KV), None, "tp"),
        ),
        check_vma=False,
    )
```

```python
import functools

import jax
import jax.numpy as jnp
from jax import lax
from jax.experimental import pallas as pl
from jax.experimental.pallas import tpu as pltpu
from jax.sharding import PartitionSpec as P

D = 2048
CONV = 4
WIDTH = 2048
EPS = 1e-05
KV = ("kz", "ky")
NEAR = 4

F32 = jnp.float32
BF16 = jnp.bfloat16
LANES = 128
VMEM = pltpu.VMEM
NT = (((1,), (1,)), ((), ()))


def local(x):
    return pltpu.with_memory_space_constraint(x, VMEM)


def lane_of(shape):
    return lax.broadcasted_iota(jnp.int32, shape, 1)


def halves(x):
    high = x.astype(BF16).astype(F32)
    return high, x - high


def project_kernel(tok, gain, wg, wv, wk, wq, ws, *rest):
    outs, (x_s, ws_s) = rest[:-2], rest[-2:]
    near = len(outs)
    seqs, prop, _ = tok.shape
    block = outs[0].shape[0]
    far = seqs // near
    here = lax.axis_index("ky")
    for k in range(near):
        place = lax.rem(here + k, near)
        for z in range(far):
            at = prop * (k * far + z)
            x_s[at : at + prop, :] = tok[z * near + place].astype(F32)
    ws_s[...] = jnp.zeros(ws_s.shape, BF16)
    ws_s[: ws.shape[0], :] = ws[...]
    x = x_s[...]
    squares = jnp.sum(x * x, axis=1, keepdims=True)
    normed = (x * gain[...]).astype(BF16)

    def put(at, product):
        width = product.shape[1]
        rounded = product.astype(BF16)
        for k, out in enumerate(outs):
            out[:, at : at + width] = rounded[block * k : block * (k + 1)]

    at = 0
    for w in (wg, wv, wk, wq):
        for c in range(0, w.shape[1], 256):
            put(at, jnp.dot(normed, w[:, c : c + 256], preferred_element_type=F32))
            at += 256
    heads = ws.shape[0]
    extra = lax.dot_general(normed, ws_s[...], NT, preferred_element_type=F32)
    put(at, with_squares(extra, squares, heads))


def with_squares(extra, squares, at):
    high, low = halves(squares)
    lane = lane_of(extra.shape)
    return jnp.where(lane == at, high, jnp.where(lane == at + 1, low, extra))


def project(tokens, gain, weights, near):
    seqs, prop, feat = tokens.shape
    columns = sum(w.shape[1] for w in weights[:4]) + LANES
    return pl.pallas_call(
        project_kernel,
        out_specs=[pl.BlockSpec(memory_space=VMEM)] * near,
        out_shape=[VMEM((seqs // near * prop, columns), BF16)] * near,
        scratch_shapes=[VMEM((seqs * prop, feat), F32), VMEM((LANES, feat), BF16)],
        name="project",
    )(tokens, gain.reshape(1, feat), *weights[:4], weights[4].T)


def fold_kernel(heads, order, *refs):
    *arrived, out = refs
    _, columns = arrived[0].shape
    _, prop, _ = out.shape
    for at in range(0, columns, LANES):
        total = arrived[0][:, at : at + LANES].astype(F32)
        for block in arrived[1:]:
            total = total + block[:, at : at + LANES].astype(F32)
        if at == columns - LANES:
            squares = total[:, heads : heads + 1] + total[:, heads + 1 : heads + 2]
            total = with_squares(total, squares, heads)
        for k, place in enumerate(order):
            out[k, :, at : at + LANES] = total[prop * place : prop * (place + 1)].astype(BF16)


def fold(arrived, order, heads):
    rows, columns = arrived[0].shape
    far = len(order)
    vmem = pl.BlockSpec(memory_space=VMEM)
    return pl.pallas_call(
        functools.partial(fold_kernel, heads, order),
        in_specs=[vmem] * len(arrived),
        out_specs=vmem,
        out_shape=VMEM((far, rows // far, columns), BF16),
        name="fold",
    )(*map(local, arrived))


def prepare_kernel(
    accepted,
    states,
    past_v,
    past_k,
    past_q,
    taps_v,
    taps_k,
    taps_q,
    bias,
    log_rate,
    out_gain,
    state,
    state_high,
    state_low,
    rows,
    base,
    taps,
    bias_out,
    rate,
    gain,
    sem,
):
    offset = accepted[0]
    fetch = pltpu.make_async_copy(states.at[0, pl.ds(offset, 1)], state, sem)
    fetch.start()
    span, prop = rows.shape[0], base.shape[0]
    at = 0
    for past, tap in ((past_v, taps_v), (past_k, taps_k), (past_q, taps_q)):
        width = past.shape[2]
        history = past[0].astype(F32)
        picked = history[0:span]
        for j in range(1, history.shape[0] - span + 1):
            picked = jnp.where(offset == j, history[j : j + span], picked)
        weight = tap[...].astype(F32)
        rows[:, at : at + width] = picked
        taps[:, at : at + width] = weight
        for t in range(prop):
            part = jnp.zeros((1, width), F32)
            for i in range(CONV):
                if t + i < span:
                    part = part + picked[t + i : t + i + 1] * weight[i : i + 1]
            base[t : t + 1, at : at + width] = part
        at += width
    bias_out[...] = bias[...]
    rate[...] = -jnp.exp(log_rate[...])
    gain[...] = out_gain[...]
    fetch.wait()
    for h in range(state.shape[1]):
        at = slice(h * state.shape[2], (h + 1) * state.shape[2])
        high = state[0, h].astype(BF16)
        state_high[at] = high
        state_low[at] = (state[0, h] - high.astype(F32)).astype(BF16)


def prepare(accepted, states, pasts, taps, bias, log_rate, out_gain):
    _, _, heads, head_dim, state_dim = states.shape
    inner = heads * head_dim
    width = sum(p.shape[2] for p in pasts)
    prop = pasts[0].shape[1] - (CONV - 1)
    plain, vmem = pl.BlockSpec(), pl.BlockSpec(memory_space=VMEM)
    return pl.pallas_call(
        prepare_kernel,
        in_specs=[pl.BlockSpec(memory_space=pltpu.SMEM), pl.BlockSpec(memory_space=pl.ANY), *[plain] * 9],
        out_specs=[vmem] * 9,
        out_shape=[
            VMEM((1, heads, head_dim, state_dim), F32),
            VMEM((inner, state_dim), BF16),
            VMEM((inner, state_dim), BF16),
            VMEM((CONV - 1, width), F32),
            VMEM((prop, width), F32),
            VMEM((CONV, width), F32),
            VMEM((1, heads), F32),
            VMEM((1, heads), F32),
            VMEM((1, inner), F32),
        ],
        scratch_shapes=[pltpu.SemaphoreType.DMA(())],
        name="prepare",
    )(
        accepted,
        states,
        *pasts,
        *taps,
        bias.reshape(1, heads),
        log_rate.reshape(1, heads),
        out_gain.reshape(1, inner),
    )


def chain_kernel(
    arrived, state_high, state_low, base, taps, bias, rate, gain, sent, moved_out, key_out, decay_out, new_out
):
    copies, prop, _ = arrived.shape
    inner, state_dim = state_high.shape
    heads = bias.shape[1]
    head_dim = inner // heads
    width = base.shape[1]
    kwidth = (width - inner) // 2
    groups = kwidth // state_dim
    per_group = inner // groups

    total = arrived[0].astype(F32)
    for i in range(1, copies):
        total = total + arrived[i].astype(F32)
    at_step = inner + width
    squares = total[:, at_step + heads : at_step + heads + 1] + total[:, at_step + heads + 1 : at_step + heads + 2]
    rscale = lax.rsqrt(squares / D + EPS)

    def scaled(start, stop):
        return (total[:, start:stop] * rscale).astype(BF16).astype(F32)

    new = scaled(inner, at_step)
    new_out[...] = new
    filtered = base[...] + new * taps[CONV - 1 : CONV]
    for i in range(1, CONV):
        later = jnp.concatenate([jnp.zeros((i, width), F32), new[: prop - i]], axis=0)
        filtered = filtered + later * taps[CONV - 1 - i : CONV - i]
    convolved = filtered / (1.0 + jnp.exp(-filtered))
    conv_v, conv_k, conv_q = convolved[:, :inner], convolved[:, inner : inner + kwidth], convolved[:, inner + kwidth :]

    raw = total[:, at_step : at_step + heads] * rscale + bias[...]
    steps = jnp.maximum(raw, 0.0) + jnp.log1p(jnp.exp(-jnp.abs(raw)))
    decay = jnp.exp(steps * rate[...])
    first_half = lane_of((prop, 2 * head_dim)) < head_dim

    def spread(x):
        return jnp.concatenate(
            [jnp.where(first_half, x[:, h : h + 1], x[:, h + 1 : h + 2]) for h in range(0, heads, 2)], axis=1
        )

    moved = spread(steps) * conv_v
    shrink = spread(decay)
    moved_out[0:prop, :] = moved
    moved_out[prop:, :] = jnp.zeros((moved_out.shape[0] - prop, inner), F32)
    key_out[...] = conv_k
    decay_out[...] = decay

    q_high, q_low = halves(conv_q)
    q_both = jnp.concatenate([q_high, q_low], axis=0).astype(BF16)
    row = lax.broadcasted_iota(jnp.int32, (prop, per_group), 0)
    ys = []
    for g in range(groups):
        cols = slice(g * per_group, (g + 1) * per_group)
        part = slice(g * state_dim, (g + 1) * state_dim)
        main = lax.dot_general(q_both[:, part], state_high[cols], NT, preferred_element_type=F32)
        rest = lax.dot_general(q_both[:prop, part], state_low[cols], NT, preferred_element_type=F32)
        carried = main[:prop] + main[prop:] + rest
        y = jnp.zeros((prop, per_group), F32)
        for t in range(prop):
            match = jnp.sum(conv_q[:, part] * conv_k[t : t + 1, part], axis=1, keepdims=True)
            carried = carried * shrink[t : t + 1, cols] + moved[t : t + 1, cols] * match
            y = jnp.where(row == t, carried, y)
        ys.append(y)
    y = jnp.concatenate(ys, axis=1)
    gate = scaled(0, inner)
    u = (y * (gate / (1.0 + jnp.exp(-gate))) * gain[...]).astype(BF16)
    for i in range(sent.shape[0]):
        sent[i] = u


def chain(copies, arrived, state_high, state_low, base, taps, bias, rate, gain):
    prop = arrived.shape[1]
    inner, heads, width = state_high.shape[0], bias.shape[1], base.shape[1]
    vmem = pl.BlockSpec(memory_space=VMEM)
    return pl.pallas_call(
        chain_kernel,
        in_specs=[vmem] * 8,
        out_specs=[vmem] * 5,
        out_shape=[
            VMEM((copies, prop, inner), BF16),
            VMEM((8, inner), F32),
            VMEM((prop, (width - inner) // 2), F32),
            VMEM((prop, heads), F32),
            VMEM((prop, width), F32),
        ],
        name="chain",
    )(*map(local, (arrived, state_high, state_low, base, taps, bias, rate, gain)))


def states_kernel(
    first, moved, keys, decay, rows, new, new_states, new_v, new_k, new_q, state_s, moved_s, sem_out
):
    prop, heads = decay.shape
    _, _, head_dim, state_dim = state_s.shape
    inner, kwidth = moved.shape[1], keys.shape[1]
    per_group = heads * state_dim // kwidth
    writes = []

    def write(source, slot):
        copy = pltpu.make_async_copy(source, new_states.at[0, slot], sem_out.at[slot])
        copy.start()
        writes.append(copy)

    write(first.at[0], 0)
    at = 0
    for out in (new_v, new_k, new_q):
        width = out.shape[2]
        both = jnp.concatenate([rows[:, at : at + width], new[:, at : at + width]], axis=0)
        out[0] = both.astype(BF16)
        at += width
    for c in range(0, inner, LANES):
        moved_s[c : c + LANES, :] = jnp.transpose(moved[:, c : c + LANES])
    for t in range(prop):
        for h in range(heads):
            g = h // per_group
            before = first[0, h] if t == 0 else state_s[t - 1, h]
            key_row = keys[t : t + 1, g * state_dim : (g + 1) * state_dim]
            column = moved_s[h * head_dim : (h + 1) * head_dim, t : t + 1]
            state_s[t, h] = before * decay[t : t + 1, h : h + 1] + column * key_row
        write(state_s.at[t], t + 1)
    for copy in writes:
        copy.wait()


def next_states(keep, first, moved, keys, decay, rows, new):
    _, heads, head_dim, state_dim = first.shape
    inner, kwidth = moved.shape[1], keys.shape[1]
    count = rows.shape[0] + new.shape[0]
    plain = pl.BlockSpec()
    vmem = pl.BlockSpec(memory_space=VMEM)
    return pl.pallas_call(
        states_kernel,
        in_specs=[vmem] * 6,
        out_specs=[pl.BlockSpec(memory_space=pl.ANY), plain, plain, plain],
        out_shape=[
            jax.ShapeDtypeStruct((1, keep, heads, head_dim, state_dim), F32),
            jax.ShapeDtypeStruct((1, count, inner), BF16),
            jax.ShapeDtypeStruct((1, count, kwidth), BF16),
            jax.ShapeDtypeStruct((1, count, kwidth), BF16),
        ],
        scratch_shapes=[
            VMEM((keep - 1, heads, head_dim, state_dim), F32),
            VMEM((inner, 8), F32),
            pltpu.SemaphoreType.DMA((keep,)),
        ],
        name="states",
    )(*map(local, (first, moved, keys, decay, rows, new)))


def output_kernel(rows, w_out, gain, out):
    features = w_out.shape[0]
    x = rows[...]
    out[:, :features] = lax.dot_general(x, w_out[...], NT, preferred_element_type=F32).astype(BF16)
    wide = x.astype(F32)
    inverse = 1.0 / (gain[...] * gain[...])
    squares = jnp.sum(wide * wide * inverse, axis=1, keepdims=True)
    high, low = halves(squares)
    lane = lane_of((x.shape[0], LANES - features))
    out[:, features:] = jnp.where(lane == 0, high, jnp.where(lane == 1, low, 0.0)).astype(BF16)


def output(rows, w_out, gain):
    vmem = pl.BlockSpec(memory_space=VMEM)
    return pl.pallas_call(
        output_kernel,
        in_specs=[vmem] * 3,
        out_specs=vmem,
        out_shape=VMEM((rows.shape[0], LANES), BF16),
        name="output",
    )(local(rows), local(w_out.T), local(gain))


def combine_kernel(order, mine, other, out):
    _, prop, features = out.shape
    a, b = mine[...].astype(F32), other[...].astype(F32)
    squares_a = a[:, features : features + 1] + a[:, features + 1 : features + 2]
    squares_b = b[:, features : features + 1] + b[:, features + 1 : features + 2]
    scale = lax.rsqrt((squares_a + squares_b) / WIDTH + EPS)
    mixed = (a[:, :features] + b[:, :features]) * scale
    for i, seq in enumerate(order):
        out[seq] = mixed[prop * i : prop * (i + 1)].astype(BF16)


def combine(mine, other, order, features):
    seqs = len(order)
    vmem = pl.BlockSpec(memory_space=VMEM)
    return pl.pallas_call(
        functools.partial(combine_kernel, order),
        in_specs=[vmem, vmem],
        out_shape=jax.ShapeDtypeStruct((seqs, mine.shape[0] // seqs, features), BF16),
        name="combine",
    )(local(mine), local(other))


def per_device(
    tokens,
    in_gain,
    w_gate,
    w_value,
    w_key,
    w_query,
    w_step,
    conv_value,
    conv_key,
    conv_query,
    step_bias,
    decay_log,
    out_gain,
    w_out,
    past_value,
    past_key,
    past_query,
    past_states,
    accepted,
):
    group_seqs, proposals, features = tokens.shape
    near, far = lax.axis_size("ky"), lax.axis_size("kz")
    near_order = [(near // 2 + i) % near for i in range(near)]
    far_order = [(far // 2 + i) % far for i in range(far)]
    order = [z * near + y for z in far_order for y in near_order]
    weights = (w_gate, w_value, w_key, w_query, w_step)
    own, *others = project(tokens, in_gain, weights, near)
    nearby = {0: own}
    for k in sorted(range(1, near), key=lambda k: -min(k, near - k)):
        nearby[k] = lax.ppermute(others[k - 1], "ky", [(i, (i + k) % near) for i in range(near)])
    first, high, low, rows, base, taps, bias, rate, gain = prepare(
        accepted,
        past_states,
        (past_value, past_key, past_query),
        (conv_value, conv_key, conv_query),
        step_bias,
        decay_log,
        out_gain,
    )
    partial = fold([nearby[k] for k in range(near)], far_order, w_step.shape[1])
    arrived = lax.all_to_all(partial, "kz", 0, 0, axis_index_groups=[far_order], tiled=True)
    sent, moved, keys, decay, new = chain(group_seqs, arrived, high, low, base, taps, bias, rate, gain)
    gathered = lax.all_to_all(sent, KV, 0, 0, axis_index_groups=[order], tiled=True)
    saved = next_states(past_states.shape[1], first, moved, keys, decay, rows, new)
    mine = output(gathered.reshape(group_seqs * proposals, -1), w_out, gain)
    swap = [(i, 1 - i) for i in range(2)]
    mixed = combine(mine, lax.ppermute(mine, "tp", swap), order, features)
    return (mixed, *saved)


def solution(mesh):
    dp, kv, tp = mesh.devices.shape
    near = NEAR if kv % NEAR == 0 else 1
    split = jax.sharding.Mesh(mesh.devices.reshape(dp, kv // near, near, tp), ("dp", *KV, "tp"))
    placed = (
        P("dp", None, KV),
        P(KV),
        P(KV, "tp"),
        P(KV, "tp"),
        P(KV, "tp"),
        P(KV, "tp"),
        P(KV, "tp"),
        P(None, "tp"),
        P(None, "tp"),
        P(None, "tp"),
        P("tp"),
        P("tp"),
        P("tp"),
        P("tp", KV),
        P(("dp", *KV), None, "tp"),
        P(("dp", *KV), None, "tp"),
        P(("dp", *KV), None, "tp"),
        P(("dp", *KV), None, "tp", None, None),
        P(("dp", *KV)),
    )
    return jax.shard_map(
        per_device,
        mesh=split,
        in_specs=placed,
        out_specs=(
            P("dp", None, KV),
            P(("dp", *KV), None, "tp", None, None),
            P(("dp", *KV), None, "tp"),
            P(("dp", *KV), None, "tp"),
            P(("dp", *KV), None, "tp"),
        ),
        check_vma=False,
    )
```

```python
import functools

import jax
import jax.numpy as jnp
from jax import lax
from jax.experimental import pallas as pl
from jax.experimental.pallas import tpu as pltpu
from jax.sharding import PartitionSpec as P

D = 2048
CONV = 4
WIDTH = 2048
EPS = 1e-05
KV = ("kz", "ky")
NEAR = 4

F32 = jnp.float32
BF16 = jnp.bfloat16
LANES = 128
VMEM = pltpu.VMEM
NT = (((1,), (1,)), ((), ()))


def local(x):
    return pltpu.with_memory_space_constraint(x, VMEM)


def lane_of(shape):
    return lax.broadcasted_iota(jnp.int32, shape, 1)


def halves(x):
    high = x.astype(BF16).astype(F32)
    return high, x - high


def project_kernel(tok, gain, wg, wv, wk, wq, ws, *rest):
    outs, (x_s, ws_s) = rest[:-2], rest[-2:]
    near = len(outs)
    seqs, prop, _ = tok.shape
    block = outs[0].shape[0]
    far = seqs // near
    here = lax.axis_index("ky")
    for k in range(near):
        place = lax.rem(here + k, near)
        for z in range(far):
            at = prop * (k * far + z)
            x_s[at : at + prop, :] = tok[z * near + place].astype(F32)
    ws_s[...] = jnp.zeros(ws_s.shape, BF16)
    ws_s[: ws.shape[0], :] = ws[...]
    x = x_s[...]
    squares = jnp.sum(x * x, axis=1, keepdims=True)
    normed = (x * gain[...]).astype(BF16)

    def put(at, product):
        width = product.shape[1]
        rounded = product.astype(BF16)
        for k, out in enumerate(outs):
            out[:, at : at + width] = rounded[block * k : block * (k + 1)]

    at = 0
    for w in (wg, wv, wk, wq):
        for c in range(0, w.shape[1], 256):
            put(at, jnp.dot(normed, w[:, c : c + 256], preferred_element_type=F32))
            at += 256
    heads = ws.shape[0]
    extra = lax.dot_general(normed, ws_s[...], NT, preferred_element_type=F32)
    put(at, with_squares(extra, squares, heads))


def with_squares(extra, squares, at):
    high, low = halves(squares)
    lane = lane_of(extra.shape)
    return jnp.where(lane == at, high, jnp.where(lane == at + 1, low, extra))


def project(tokens, gain, weights, near):
    seqs, prop, feat = tokens.shape
    columns = sum(w.shape[1] for w in weights[:4]) + LANES
    return pl.pallas_call(
        project_kernel,
        out_specs=[pl.BlockSpec(memory_space=VMEM)] * near,
        out_shape=[VMEM((seqs // near * prop, columns), BF16)] * near,
        scratch_shapes=[VMEM((seqs * prop, feat), F32), VMEM((LANES, feat), BF16)],
        name="project",
    )(tokens, gain.reshape(1, feat), *weights[:4], weights[4].T)


def fold_kernel(heads, order, *refs):
    *arrived, out = refs
    _, columns = arrived[0].shape
    _, prop, _ = out.shape
    for at in range(0, columns, LANES):
        total = arrived[0][:, at : at + LANES].astype(F32)
        for block in arrived[1:]:
            total = total + block[:, at : at + LANES].astype(F32)
        if at == columns - LANES:
            squares = total[:, heads : heads + 1] + total[:, heads + 1 : heads + 2]
            total = with_squares(total, squares, heads)
        for k, place in enumerate(order):
            out[k, :, at : at + LANES] = total[prop * place : prop * (place + 1)].astype(BF16)


def fold(arrived, order, heads):
    rows, columns = arrived[0].shape
    far = len(order)
    vmem = pl.BlockSpec(memory_space=VMEM)
    return pl.pallas_call(
        functools.partial(fold_kernel, heads, order),
        in_specs=[vmem] * len(arrived),
        out_specs=vmem,
        out_shape=VMEM((far, rows // far, columns), BF16),
        name="fold",
    )(*map(local, arrived))


def prepare_kernel(
    accepted,
    states,
    past_v,
    past_k,
    past_q,
    taps_v,
    taps_k,
    taps_q,
    bias,
    log_rate,
    out_gain,
    state,
    state_high,
    state_low,
    rows,
    base,
    taps,
    bias_out,
    rate,
    gain,
    sem,
):
    offset = accepted[0]
    fetch = pltpu.make_async_copy(states.at[0, pl.ds(offset, 1)], state, sem)
    fetch.start()
    span, prop = rows.shape[0], base.shape[0]
    at = 0
    for past, tap in ((past_v, taps_v), (past_k, taps_k), (past_q, taps_q)):
        width = past.shape[2]
        history = past[0].astype(F32)
        picked = history[0:span]
        for j in range(1, history.shape[0] - span + 1):
            picked = jnp.where(offset == j, history[j : j + span], picked)
        weight = tap[...].astype(F32)
        rows[:, at : at + width] = picked
        taps[:, at : at + width] = weight
        for t in range(prop):
            part = jnp.zeros((1, width), F32)
            for i in range(CONV):
                if t + i < span:
                    part = part + picked[t + i : t + i + 1] * weight[i : i + 1]
            base[t : t + 1, at : at + width] = part
        at += width
    bias_out[...] = bias[...]
    rate[...] = -jnp.exp(log_rate[...])
    gain[...] = out_gain[...]
    fetch.wait()
    for h in range(state.shape[1]):
        at = slice(h * state.shape[2], (h + 1) * state.shape[2])
        high = state[0, h].astype(BF16)
        state_high[at] = high
        state_low[at] = (state[0, h] - high.astype(F32)).astype(BF16)


def prepare(accepted, states, pasts, taps, bias, log_rate, out_gain):
    _, _, heads, head_dim, state_dim = states.shape
    inner = heads * head_dim
    width = sum(p.shape[2] for p in pasts)
    prop = pasts[0].shape[1] - (CONV - 1)
    plain, vmem = pl.BlockSpec(), pl.BlockSpec(memory_space=VMEM)
    return pl.pallas_call(
        prepare_kernel,
        in_specs=[pl.BlockSpec(memory_space=pltpu.SMEM), pl.BlockSpec(memory_space=pl.ANY), *[plain] * 9],
        out_specs=[vmem] * 9,
        out_shape=[
            VMEM((1, heads, head_dim, state_dim), F32),
            VMEM((inner, state_dim), BF16),
            VMEM((inner, state_dim), BF16),
            VMEM((CONV - 1, width), F32),
            VMEM((prop, width), F32),
            VMEM((CONV, width), F32),
            VMEM((1, heads), F32),
            VMEM((1, heads), F32),
            VMEM((1, inner), F32),
        ],
        scratch_shapes=[pltpu.SemaphoreType.DMA(())],
        name="prepare",
    )(
        accepted,
        states,
        *pasts,
        *taps,
        bias.reshape(1, heads),
        log_rate.reshape(1, heads),
        out_gain.reshape(1, inner),
    )


def chain_kernel(
    arrived, state_high, state_low, base, taps, bias, rate, gain, sent, moved_out, key_out, decay_out, new_out
):
    copies, prop, _ = arrived.shape
    inner, state_dim = state_high.shape
    heads = bias.shape[1]
    head_dim = inner // heads
    width = base.shape[1]
    kwidth = (width - inner) // 2
    groups = kwidth // state_dim
    per_group = inner // groups

    total = arrived[0].astype(F32)
    for i in range(1, copies):
        total = total + arrived[i].astype(F32)
    at_step = inner + width
    squares = total[:, at_step + heads : at_step + heads + 1] + total[:, at_step + heads + 1 : at_step + heads + 2]
    rscale = lax.rsqrt(squares / D + EPS)

    def scaled(start, stop):
        return (total[:, start:stop] * rscale).astype(BF16).astype(F32)

    new = scaled(inner, at_step)
    new_out[...] = new
    filtered = base[...] + new * taps[CONV - 1 : CONV]
    for i in range(1, CONV):
        later = jnp.concatenate([jnp.zeros((i, width), F32), new[: prop - i]], axis=0)
        filtered = filtered + later * taps[CONV - 1 - i : CONV - i]
    convolved = filtered / (1.0 + jnp.exp(-filtered))
    conv_v, conv_k, conv_q = convolved[:, :inner], convolved[:, inner : inner + kwidth], convolved[:, inner + kwidth :]

    raw = total[:, at_step : at_step + heads] * rscale + bias[...]
    steps = jnp.maximum(raw, 0.0) + jnp.log1p(jnp.exp(-jnp.abs(raw)))
    decay = jnp.exp(steps * rate[...])
    first_half = lane_of((prop, 2 * head_dim)) < head_dim

    def spread(x):
        return jnp.concatenate(
            [jnp.where(first_half, x[:, h : h + 1], x[:, h + 1 : h + 2]) for h in range(0, heads, 2)], axis=1
        )

    moved = spread(steps) * conv_v
    shrink = spread(decay)
    moved_out[0:prop, :] = moved
    moved_out[prop:, :] = jnp.zeros((moved_out.shape[0] - prop, inner), F32)
    key_out[...] = conv_k
    decay_out[...] = decay

    q_high, q_low = halves(conv_q)
    q_both = jnp.concatenate([q_high, q_low], axis=0).astype(BF16)
    row = lax.broadcasted_iota(jnp.int32, (prop, per_group), 0)
    ys = []
    for g in range(groups):
        cols = slice(g * per_group, (g + 1) * per_group)
        part = slice(g * state_dim, (g + 1) * state_dim)
        main = lax.dot_general(q_both[:, part], state_high[cols], NT, preferred_element_type=F32)
        rest = lax.dot_general(q_both[:prop, part], state_low[cols], NT, preferred_element_type=F32)
        carried = main[:prop] + main[prop:] + rest
        y = jnp.zeros((prop, per_group), F32)
        for t in range(prop):
            match = jnp.sum(conv_q[:, part] * conv_k[t : t + 1, part], axis=1, keepdims=True)
            carried = carried * shrink[t : t + 1, cols] + moved[t : t + 1, cols] * match
            y = jnp.where(row == t, carried, y)
        ys.append(y)
    y = jnp.concatenate(ys, axis=1)
    gate = scaled(0, inner)
    u = (y * (gate / (1.0 + jnp.exp(-gate))) * gain[...]).astype(BF16)
    for i in range(sent.shape[0]):
        sent[i] = u


def chain(copies, arrived, state_high, state_low, base, taps, bias, rate, gain):
    prop = arrived.shape[1]
    inner, heads, width = state_high.shape[0], bias.shape[1], base.shape[1]
    vmem = pl.BlockSpec(memory_space=VMEM)
    return pl.pallas_call(
        chain_kernel,
        in_specs=[vmem] * 8,
        out_specs=[vmem] * 5,
        out_shape=[
            VMEM((copies, prop, inner), BF16),
            VMEM((8, inner), F32),
            VMEM((prop, (width - inner) // 2), F32),
            VMEM((prop, heads), F32),
            VMEM((prop, width), F32),
        ],
        name="chain",
    )(*map(local, (arrived, state_high, state_low, base, taps, bias, rate, gain)))


def states_kernel(
    first, moved, keys, decay, rows, new, new_states, new_v, new_k, new_q, state_s, moved_s, sem_out
):
    prop, heads = decay.shape
    _, _, head_dim, state_dim = state_s.shape
    inner, kwidth = moved.shape[1], keys.shape[1]
    per_group = heads * state_dim // kwidth
    writes = []

    def write(source, slot):
        copy = pltpu.make_async_copy(source, new_states.at[0, slot], sem_out.at[slot])
        copy.start()
        writes.append(copy)

    write(first.at[0], 0)
    at = 0
    for out in (new_v, new_k, new_q):
        width = out.shape[2]
        both = jnp.concatenate([rows[:, at : at + width], new[:, at : at + width]], axis=0)
        out[0] = both.astype(BF16)
        at += width
    for c in range(0, inner, LANES):
        moved_s[c : c + LANES, :] = jnp.transpose(moved[:, c : c + LANES])
    for t in range(prop):
        for h in range(heads):
            g = h // per_group
            before = first[0, h] if t == 0 else state_s[t - 1, h]
            key_row = keys[t : t + 1, g * state_dim : (g + 1) * state_dim]
            column = moved_s[h * head_dim : (h + 1) * head_dim, t : t + 1]
            state_s[t, h] = before * decay[t : t + 1, h : h + 1] + column * key_row
        write(state_s.at[t], t + 1)
    for copy in writes:
        copy.wait()


def next_states(keep, first, moved, keys, decay, rows, new):
    _, heads, head_dim, state_dim = first.shape
    inner, kwidth = moved.shape[1], keys.shape[1]
    count = rows.shape[0] + new.shape[0]
    plain = pl.BlockSpec()
    vmem = pl.BlockSpec(memory_space=VMEM)
    return pl.pallas_call(
        states_kernel,
        in_specs=[vmem] * 6,
        out_specs=[pl.BlockSpec(memory_space=pl.ANY), plain, plain, plain],
        out_shape=[
            jax.ShapeDtypeStruct((1, keep, heads, head_dim, state_dim), F32),
            jax.ShapeDtypeStruct((1, count, inner), BF16),
            jax.ShapeDtypeStruct((1, count, kwidth), BF16),
            jax.ShapeDtypeStruct((1, count, kwidth), BF16),
        ],
        scratch_shapes=[
            VMEM((keep - 1, heads, head_dim, state_dim), F32),
            VMEM((inner, 8), F32),
            pltpu.SemaphoreType.DMA((keep,)),
        ],
        name="states",
    )(*map(local, (first, moved, keys, decay, rows, new)))


def output_kernel(rows, w_out, gain, out):
    features = w_out.shape[0]
    x = rows[...]
    out[:, :features] = lax.dot_general(x, w_out[...], NT, preferred_element_type=F32).astype(BF16)
    wide = x.astype(F32)
    inverse = 1.0 / (gain[...] * gain[...])
    squares = jnp.sum(wide * wide * inverse, axis=1, keepdims=True)
    high, low = halves(squares)
    lane = lane_of((x.shape[0], LANES - features))
    out[:, features:] = jnp.where(lane == 0, high, jnp.where(lane == 1, low, 0.0)).astype(BF16)


def output(rows, w_out, gain):
    vmem = pl.BlockSpec(memory_space=VMEM)
    return pl.pallas_call(
        output_kernel,
        in_specs=[vmem] * 3,
        out_specs=vmem,
        out_shape=VMEM((rows.shape[0], LANES), BF16),
        name="output",
    )(local(rows), local(w_out.T), local(gain))


def combine_kernel(order, mine, other, out):
    _, prop, features = out.shape
    a, b = mine[...].astype(F32), other[...].astype(F32)
    squares_a = a[:, features : features + 1] + a[:, features + 1 : features + 2]
    squares_b = b[:, features : features + 1] + b[:, features + 1 : features + 2]
    scale = lax.rsqrt((squares_a + squares_b) / WIDTH + EPS)
    mixed = (a[:, :features] + b[:, :features]) * scale
    for i, seq in enumerate(order):
        out[seq] = mixed[prop * i : prop * (i + 1)].astype(BF16)


def combine(mine, other, order, features):
    seqs = len(order)
    vmem = pl.BlockSpec(memory_space=VMEM)
    return pl.pallas_call(
        functools.partial(combine_kernel, order),
        in_specs=[vmem, vmem],
        out_shape=jax.ShapeDtypeStruct((seqs, mine.shape[0] // seqs, features), BF16),
        name="combine",
    )(local(mine), local(other))


def per_device(
    tokens,
    in_gain,
    w_gate,
    w_value,
    w_key,
    w_query,
    w_step,
    conv_value,
    conv_key,
    conv_query,
    step_bias,
    decay_log,
    out_gain,
    w_out,
    past_value,
    past_key,
    past_query,
    past_states,
    accepted,
):
    group_seqs, proposals, features = tokens.shape
    near, far = lax.axis_size("ky"), lax.axis_size("kz")
    far_order = [(far // 2 + 1 + i) % far for i in range(far)]
    order = [(far // 2 + i) % far * near + (near // 2 + j) % near for i in range(far) for j in range(near)]
    weights = (w_gate, w_value, w_key, w_query, w_step)
    own, *others = project(tokens, in_gain, weights, near)
    nearby = {0: own}
    for k in sorted(range(1, near), key=lambda k: -min(k, near - k)):
        nearby[k] = lax.ppermute(others[k - 1], "ky", [(i, (i + k) % near) for i in range(near)])
    first, high, low, rows, base, taps, bias, rate, gain = prepare(
        accepted,
        past_states,
        (past_value, past_key, past_query),
        (conv_value, conv_key, conv_query),
        step_bias,
        decay_log,
        out_gain,
    )
    partial = fold([nearby[k] for k in range(near)], far_order, w_step.shape[1])
    arrived = lax.all_to_all(partial, "kz", 0, 0, axis_index_groups=[far_order], tiled=True)
    sent, moved, keys, decay, new = chain(group_seqs, arrived, high, low, base, taps, bias, rate, gain)
    gathered = lax.all_to_all(sent, KV, 0, 0, axis_index_groups=[order], tiled=True)
    saved = next_states(past_states.shape[1], first, moved, keys, decay, rows, new)
    mine = output(gathered.reshape(group_seqs * proposals, -1), w_out, gain)
    swap = [(i, 1 - i) for i in range(2)]
    mixed = combine(mine, lax.ppermute(mine, "tp", swap), order, features)
    return (mixed, *saved)


def solution(mesh):
    dp, kv, tp = mesh.devices.shape
    near = NEAR if kv % NEAR == 0 else 1
    split = jax.sharding.Mesh(mesh.devices.reshape(dp, kv // near, near, tp), ("dp", *KV, "tp"))
    placed = (
        P("dp", None, KV),
        P(KV),
        P(KV, "tp"),
        P(KV, "tp"),
        P(KV, "tp"),
        P(KV, "tp"),
        P(KV, "tp"),
        P(None, "tp"),
        P(None, "tp"),
        P(None, "tp"),
        P("tp"),
        P("tp"),
        P("tp"),
        P("tp", KV),
        P(("dp", *KV), None, "tp"),
        P(("dp", *KV), None, "tp"),
        P(("dp", *KV), None, "tp"),
        P(("dp", *KV), None, "tp", None, None),
        P(("dp", *KV)),
    )
    return jax.shard_map(
        per_device,
        mesh=split,
        in_specs=placed,
        out_specs=(
            P("dp", None, KV),
            P(("dp", *KV), None, "tp", None, None),
            P(("dp", *KV), None, "tp"),
            P(("dp", *KV), None, "tp"),
            P(("dp", *KV), None, "tp"),
        ),
        check_vma=False,
    )
```

```python
import functools

import jax
import jax.numpy as jnp
from jax import lax
from jax.experimental import pallas as pl
from jax.experimental.pallas import tpu as pltpu
from jax.sharding import PartitionSpec as P

D = 2048
CONV = 4
WIDTH = 2048
EPS = 1e-05
KV = ("kz", "ky")
NEAR = 4

F32 = jnp.float32
BF16 = jnp.bfloat16
LANES = 128
PACK = 4
VMEM = pltpu.VMEM
NT = (((1,), (1,)), ((), ()))


def local(x):
    return pltpu.with_memory_space_constraint(x, VMEM)


def lane_of(shape):
    return lax.broadcasted_iota(jnp.int32, shape, 1)


def halves(x):
    high = x.astype(BF16).astype(F32)
    return high, x - high


def project_kernel(tok, gain, wg, wv, wk, wq, ws, *rest):
    outs, (x_s, ws_s) = rest[:-2], rest[-2:]
    near = len(outs)
    seqs, prop, _ = tok.shape
    far = seqs // near
    block = far * prop
    here = lax.axis_index("ky")
    for k in range(near):
        place = lax.rem(here + k, near)
        for z in range(far):
            at = prop * (k * far + z)
            x_s[at : at + prop, :] = tok[z * near + place].astype(F32)
    ws_s[...] = jnp.zeros(ws_s.shape, BF16)
    ws_s[: ws.shape[0], :] = ws[...]
    x = x_s[...]
    squares = jnp.sum(x * x, axis=1, keepdims=True)
    normed = (x * gain[...]).astype(BF16)

    at = 0
    for w in (wg, wv, wk, wq):
        for c in range(0, w.shape[1], 2 * LANES):
            product = jnp.dot(normed, w[:, c : c + 2 * LANES], preferred_element_type=F32).astype(BF16)
            for part in (product[:, :LANES], product[:, LANES:]):
                for k, out in enumerate(outs):
                    out[at : at + block, :] = part[block * k : block * (k + 1)]
                at += block
    heads = ws.shape[0]
    extra = lax.dot_general(normed, ws_s[...], NT, preferred_element_type=F32)
    extra = with_squares(extra, squares, heads)
    strip, wide = block // PACK, LANES // PACK
    for k, out in enumerate(outs):
        strips = [extra[block * k + strip * j : block * k + strip * (j + 1), :wide] for j in range(PACK)]
        out[at:, :] = jnp.concatenate(strips, axis=1).astype(BF16)


def with_squares(extra, squares, at):
    high, low = halves(squares)
    lane = lane_of(extra.shape)
    return jnp.where(lane == at, high, jnp.where(lane == at + 1, low, extra))


def project(tokens, gain, weights, near):
    seqs, prop, feat = tokens.shape
    block = seqs // near * prop
    rows = sum(w.shape[1] for w in weights[:4]) // LANES * block + block // PACK
    return pl.pallas_call(
        project_kernel,
        out_specs=[pl.BlockSpec(memory_space=VMEM)] * near,
        out_shape=[VMEM((rows, LANES), BF16)] * near,
        scratch_shapes=[VMEM((seqs * prop, feat), F32), VMEM((LANES, feat), BF16)],
        name="project",
    )(tokens, gain.reshape(1, feat), *weights[:4], weights[4].T)


def fold_kernel(heads, order, *refs):
    *arrived, out = refs
    far, prop, columns = out.shape
    block = far * prop
    for at in range(0, columns, LANES):
        start = at // LANES * block
        last = at == columns - LANES
        part = slice(start, start + (block // PACK if last else block))
        total = arrived[0][part].astype(F32)
        for other in arrived[1:]:
            total = total + other[part].astype(F32)
        if last:
            wide = LANES // PACK
            total = jnp.concatenate([total[:, wide * j : wide * (j + 1)] for j in range(PACK)], axis=0)
            total = jnp.concatenate([total, jnp.zeros((block, LANES - wide), F32)], axis=1)
            squares = total[:, heads : heads + 1] + total[:, heads + 1 : heads + 2]
            total = with_squares(total, squares, heads)
        for k, place in enumerate(order):
            out[k, :, at : at + LANES] = total[prop * place : prop * (place + 1)].astype(BF16)


def fold(arrived, order, prop, columns, heads):
    far = len(order)
    vmem = pl.BlockSpec(memory_space=VMEM)
    return pl.pallas_call(
        functools.partial(fold_kernel, heads, order),
        in_specs=[vmem] * len(arrived),
        out_specs=vmem,
        out_shape=VMEM((far, prop, columns), BF16),
        name="fold",
    )(*map(local, arrived))


def prepare_kernel(
    accepted,
    states,
    past_v,
    past_k,
    past_q,
    taps_v,
    taps_k,
    taps_q,
    bias,
    log_rate,
    out_gain,
    state,
    state_high,
    state_low,
    rows,
    base,
    taps,
    bias_out,
    rate,
    gain,
    sem,
):
    offset = accepted[0]
    fetch = pltpu.make_async_copy(states.at[0, pl.ds(offset, 1)], state, sem)
    fetch.start()
    span, prop = rows.shape[0], base.shape[0]
    at = 0
    for past, tap in ((past_v, taps_v), (past_k, taps_k), (past_q, taps_q)):
        width = past.shape[2]
        history = past[0].astype(F32)
        picked = history[0:span]
        for j in range(1, history.shape[0] - span + 1):
            picked = jnp.where(offset == j, history[j : j + span], picked)
        weight = tap[...].astype(F32)
        rows[:, at : at + width] = picked
        taps[:, at : at + width] = weight
        for t in range(prop):
            part = jnp.zeros((1, width), F32)
            for i in range(CONV):
                if t + i < span:
                    part = part + picked[t + i : t + i + 1] * weight[i : i + 1]
            base[t : t + 1, at : at + width] = part
        at += width
    bias_out[...] = bias[...]
    rate[...] = -jnp.exp(log_rate[...])
    gain[...] = out_gain[...]
    fetch.wait()
    for h in range(state.shape[1]):
        at = slice(h * state.shape[2], (h + 1) * state.shape[2])
        high = state[0, h].astype(BF16)
        state_high[at] = high
        state_low[at] = (state[0, h] - high.astype(F32)).astype(BF16)


def prepare(accepted, states, pasts, taps, bias, log_rate, out_gain):
    _, _, heads, head_dim, state_dim = states.shape
    inner = heads * head_dim
    width = sum(p.shape[2] for p in pasts)
    prop = pasts[0].shape[1] - (CONV - 1)
    plain, vmem = pl.BlockSpec(), pl.BlockSpec(memory_space=VMEM)
    return pl.pallas_call(
        prepare_kernel,
        in_specs=[pl.BlockSpec(memory_space=pltpu.SMEM), pl.BlockSpec(memory_space=pl.ANY), *[plain] * 9],
        out_specs=[vmem] * 9,
        out_shape=[
            VMEM((1, heads, head_dim, state_dim), F32),
            VMEM((inner, state_dim), BF16),
            VMEM((inner, state_dim), BF16),
            VMEM((CONV - 1, width), F32),
            VMEM((prop, width), F32),
            VMEM((CONV, width), F32),
            VMEM((1, heads), F32),
            VMEM((1, heads), F32),
            VMEM((1, inner), F32),
        ],
        scratch_shapes=[pltpu.SemaphoreType.DMA(())],
        name="prepare",
    )(
        accepted,
        states,
        *pasts,
        *taps,
        bias.reshape(1, heads),
        log_rate.reshape(1, heads),
        out_gain.reshape(1, inner),
    )


def chain_kernel(
    arrived, state_high, state_low, base, taps, bias, rate, gain, sent, moved_out, key_out, decay_out, new_out
):
    copies, prop, _ = arrived.shape
    inner, state_dim = state_high.shape
    heads = bias.shape[1]
    head_dim = inner // heads
    width = base.shape[1]
    kwidth = (width - inner) // 2
    groups = kwidth // state_dim
    per_group = inner // groups

    total = arrived[0].astype(F32)
    for i in range(1, copies):
        total = total + arrived[i].astype(F32)
    at_step = inner + width
    squares = total[:, at_step + heads : at_step + heads + 1] + total[:, at_step + heads + 1 : at_step + heads + 2]
    rscale = lax.rsqrt(squares / D + EPS)

    def scaled(start, stop):
        return (total[:, start:stop] * rscale).astype(BF16).astype(F32)

    new = scaled(inner, at_step)
    new_out[...] = new
    filtered = base[...] + new * taps[CONV - 1 : CONV]
    for i in range(1, CONV):
        later = jnp.concatenate([jnp.zeros((i, width), F32), new[: prop - i]], axis=0)
        filtered = filtered + later * taps[CONV - 1 - i : CONV - i]
    convolved = filtered / (1.0 + jnp.exp(-filtered))
    conv_v, conv_k, conv_q = convolved[:, :inner], convolved[:, inner : inner + kwidth], convolved[:, inner + kwidth :]

    raw = total[:, at_step : at_step + heads] * rscale + bias[...]
    steps = jnp.maximum(raw, 0.0) + jnp.log1p(jnp.exp(-jnp.abs(raw)))
    decay = jnp.exp(steps * rate[...])
    first_half = lane_of((prop, 2 * head_dim)) < head_dim

    def spread(x):
        return jnp.concatenate(
            [jnp.where(first_half, x[:, h : h + 1], x[:, h + 1 : h + 2]) for h in range(0, heads, 2)], axis=1
        )

    moved = spread(steps) * conv_v
    shrink = spread(decay)
    moved_out[0:prop, :] = moved
    moved_out[prop:, :] = jnp.zeros((moved_out.shape[0] - prop, inner), F32)
    key_out[...] = conv_k
    decay_out[...] = decay

    q_high, q_low = halves(conv_q)
    q_both = jnp.concatenate([q_high, q_low], axis=0).astype(BF16)
    row = lax.broadcasted_iota(jnp.int32, (prop, per_group), 0)
    ys = []
    for g in range(groups):
        cols = slice(g * per_group, (g + 1) * per_group)
        part = slice(g * state_dim, (g + 1) * state_dim)
        main = lax.dot_general(q_both[:, part], state_high[cols], NT, preferred_element_type=F32)
        rest = lax.dot_general(q_both[:prop, part], state_low[cols], NT, preferred_element_type=F32)
        carried = main[:prop] + main[prop:] + rest
        y = jnp.zeros((prop, per_group), F32)
        for t in range(prop):
            match = jnp.sum(conv_q[:, part] * conv_k[t : t + 1, part], axis=1, keepdims=True)
            carried = carried * shrink[t : t + 1, cols] + moved[t : t + 1, cols] * match
            y = jnp.where(row == t, carried, y)
        ys.append(y)
    y = jnp.concatenate(ys, axis=1)
    gate = scaled(0, inner)
    u = (y * (gate / (1.0 + jnp.exp(-gate))) * gain[...]).astype(BF16)
    for i in range(sent.shape[0]):
        sent[i] = u


def chain(copies, arrived, state_high, state_low, base, taps, bias, rate, gain):
    prop = arrived.shape[1]
    inner, heads, width = state_high.shape[0], bias.shape[1], base.shape[1]
    vmem = pl.BlockSpec(memory_space=VMEM)
    return pl.pallas_call(
        chain_kernel,
        in_specs=[vmem] * 8,
        out_specs=[vmem] * 5,
        out_shape=[
            VMEM((copies, prop, inner), BF16),
            VMEM((8, inner), F32),
            VMEM((prop, (width - inner) // 2), F32),
            VMEM((prop, heads), F32),
            VMEM((prop, width), F32),
        ],
        name="chain",
    )(*map(local, (arrived, state_high, state_low, base, taps, bias, rate, gain)))


def states_kernel(
    first, moved, keys, decay, rows, new, new_states, new_v, new_k, new_q, state_s, moved_s, sem_out
):
    prop, heads = decay.shape
    _, _, head_dim, state_dim = state_s.shape
    inner, kwidth = moved.shape[1], keys.shape[1]
    per_group = heads * state_dim // kwidth
    writes = []

    def write(source, slot):
        copy = pltpu.make_async_copy(source, new_states.at[0, slot], sem_out.at[slot])
        copy.start()
        writes.append(copy)

    write(first.at[0], 0)
    at = 0
    for out in (new_v, new_k, new_q):
        width = out.shape[2]
        both = jnp.concatenate([rows[:, at : at + width], new[:, at : at + width]], axis=0)
        out[0] = both.astype(BF16)
        at += width
    for c in range(0, inner, LANES):
        moved_s[c : c + LANES, :] = jnp.transpose(moved[:, c : c + LANES])
    for t in range(prop):
        for h in range(heads):
            g = h // per_group
            before = first[0, h] if t == 0 else state_s[t - 1, h]
            key_row = keys[t : t + 1, g * state_dim : (g + 1) * state_dim]
            column = moved_s[h * head_dim : (h + 1) * head_dim, t : t + 1]
            state_s[t, h] = before * decay[t : t + 1, h : h + 1] + column * key_row
        write(state_s.at[t], t + 1)
    for copy in writes:
        copy.wait()


def next_states(keep, first, moved, keys, decay, rows, new):
    _, heads, head_dim, state_dim = first.shape
    inner, kwidth = moved.shape[1], keys.shape[1]
    count = rows.shape[0] + new.shape[0]
    plain = pl.BlockSpec()
    vmem = pl.BlockSpec(memory_space=VMEM)
    return pl.pallas_call(
        states_kernel,
        in_specs=[vmem] * 6,
        out_specs=[pl.BlockSpec(memory_space=pl.ANY), plain, plain, plain],
        out_shape=[
            jax.ShapeDtypeStruct((1, keep, heads, head_dim, state_dim), F32),
            jax.ShapeDtypeStruct((1, count, inner), BF16),
            jax.ShapeDtypeStruct((1, count, kwidth), BF16),
            jax.ShapeDtypeStruct((1, count, kwidth), BF16),
        ],
        scratch_shapes=[
            VMEM((keep - 1, heads, head_dim, state_dim), F32),
            VMEM((inner, 8), F32),
            pltpu.SemaphoreType.DMA((keep,)),
        ],
        name="states",
    )(*map(local, (first, moved, keys, decay, rows, new)))


def output_kernel(rows, w_out, gain, out):
    features = w_out.shape[0]
    x = rows[...]
    out[:, :features] = lax.dot_general(x, w_out[...], NT, preferred_element_type=F32).astype(BF16)
    wide = x.astype(F32)
    inverse = 1.0 / (gain[...] * gain[...])
    squares = jnp.sum(wide * wide * inverse, axis=1, keepdims=True)
    high, low = halves(squares)
    lane = lane_of((x.shape[0], LANES - features))
    out[:, features:] = jnp.where(lane == 0, high, jnp.where(lane == 1, low, 0.0)).astype(BF16)


def output(rows, w_out, gain):
    vmem = pl.BlockSpec(memory_space=VMEM)
    return pl.pallas_call(
        output_kernel,
        in_specs=[vmem] * 3,
        out_specs=vmem,
        out_shape=VMEM((rows.shape[0], LANES), BF16),
        name="output",
    )(local(rows), local(w_out.T), local(gain))


def combine_kernel(order, mine, other, out):
    _, prop, features = out.shape
    a, b = mine[...].astype(F32), other[...].astype(F32)
    squares_a = a[:, features : features + 1] + a[:, features + 1 : features + 2]
    squares_b = b[:, features : features + 1] + b[:, features + 1 : features + 2]
    scale = lax.rsqrt((squares_a + squares_b) / WIDTH + EPS)
    mixed = (a[:, :features] + b[:, :features]) * scale
    for i, seq in enumerate(order):
        out[seq] = mixed[prop * i : prop * (i + 1)].astype(BF16)


def combine(mine, other, order, features):
    seqs = len(order)
    vmem = pl.BlockSpec(memory_space=VMEM)
    return pl.pallas_call(
        functools.partial(combine_kernel, order),
        in_specs=[vmem, vmem],
        out_shape=jax.ShapeDtypeStruct((seqs, mine.shape[0] // seqs, features), BF16),
        name="combine",
    )(local(mine), local(other))


def per_device(
    tokens,
    in_gain,
    w_gate,
    w_value,
    w_key,
    w_query,
    w_step,
    conv_value,
    conv_key,
    conv_query,
    step_bias,
    decay_log,
    out_gain,
    w_out,
    past_value,
    past_key,
    past_query,
    past_states,
    accepted,
):
    group_seqs, proposals, features = tokens.shape
    near, far = lax.axis_size("ky"), lax.axis_size("kz")
    far_order = [(far // 2 + 1 + i) % far for i in range(far)]
    order = [(far // 2 + i) % far * near + (near // 2 + j) % near for i in range(far) for j in range(near)]
    weights = (w_gate, w_value, w_key, w_query, w_step)
    columns = sum(w.shape[1] for w in weights[:4]) + LANES
    own, *others = project(tokens, in_gain, weights, near)
    nearby = {0: own}
    for k in sorted(range(1, near), key=lambda k: -min(k, near - k)):
        nearby[k] = lax.ppermute(others[k - 1], "ky", [(i, (i + k) % near) for i in range(near)])
    first, high, low, rows, base, taps, bias, rate, gain = prepare(
        accepted,
        past_states,
        (past_value, past_key, past_query),
        (conv_value, conv_key, conv_query),
        step_bias,
        decay_log,
        out_gain,
    )
    partial = fold([nearby[k] for k in range(near)], far_order, proposals, columns, w_step.shape[1])
    arrived = lax.all_to_all(partial, "kz", 0, 0, axis_index_groups=[far_order], tiled=True)
    sent, moved, keys, decay, new = chain(group_seqs, arrived, high, low, base, taps, bias, rate, gain)
    gathered = lax.all_to_all(sent, KV, 0, 0, axis_index_groups=[order], tiled=True)
    saved = next_states(past_states.shape[1], first, moved, keys, decay, rows, new)
    mine = output(gathered.reshape(group_seqs * proposals, -1), w_out, gain)
    swap = [(i, 1 - i) for i in range(2)]
    mixed = combine(mine, lax.ppermute(mine, "tp", swap), order, features)
    return (mixed, *saved)


def solution(mesh):
    dp, kv, tp = mesh.devices.shape
    near = NEAR if kv % NEAR == 0 else 1
    split = jax.sharding.Mesh(mesh.devices.reshape(dp, kv // near, near, tp), ("dp", *KV, "tp"))
    placed = (
        P("dp", None, KV),
        P(KV),
        P(KV, "tp"),
        P(KV, "tp"),
        P(KV, "tp"),
        P(KV, "tp"),
        P(KV, "tp"),
        P(None, "tp"),
        P(None, "tp"),
        P(None, "tp"),
        P("tp"),
        P("tp"),
        P("tp"),
        P("tp", KV),
        P(("dp", *KV), None, "tp"),
        P(("dp", *KV), None, "tp"),
        P(("dp", *KV), None, "tp"),
        P(("dp", *KV), None, "tp", None, None),
        P(("dp", *KV)),
    )
    return jax.shard_map(
        per_device,
        mesh=split,
        in_specs=placed,
        out_specs=(
            P("dp", None, KV),
            P(("dp", *KV), None, "tp", None, None),
            P(("dp", *KV), None, "tp"),
            P(("dp", *KV), None, "tp"),
            P(("dp", *KV), None, "tp"),
        ),
        check_vma=False,
    )
```

```python
import functools

import jax
import jax.numpy as jnp
from jax import lax
from jax.experimental import pallas as pl
from jax.experimental.pallas import tpu as pltpu
from jax.sharding import PartitionSpec as P

D = 2048
CONV = 4
WIDTH = 2048
EPS = 1e-05
KV = ("kz", "ky")
NEAR = 4

F32 = jnp.float32
BF16 = jnp.bfloat16
LANES = 128
VMEM = pltpu.VMEM
NT = (((1,), (1,)), ((), ()))


def local(x):
    return pltpu.with_memory_space_constraint(x, VMEM)


def lane_of(shape):
    return lax.broadcasted_iota(jnp.int32, shape, 1)


def halves(x):
    high = x.astype(BF16).astype(F32)
    return high, x - high


def project_kernel(tok, gain, wg, wv, wk, wq, ws, *rest):
    outs, (x_s, ws_s) = rest[:-2], rest[-2:]
    near = len(outs)
    seqs, prop, _ = tok.shape
    block = outs[0].shape[0]
    far = seqs // near
    here = lax.axis_index("ky")
    for k in range(near):
        place = lax.rem(here + k, near)
        for z in range(far):
            at = prop * (k * far + z)
            x_s[at : at + prop, :] = tok[z * near + place].astype(F32)
    ws_s[...] = jnp.zeros(ws_s.shape, BF16)
    ws_s[: ws.shape[0], :] = ws[...]
    x = x_s[...]
    squares = jnp.sum(x * x, axis=1, keepdims=True)
    normed = (x * gain[...]).astype(BF16)

    def put(at, product):
        width = product.shape[1]
        rounded = product.astype(BF16)
        for k, out in enumerate(outs):
            out[:, at : at + width] = rounded[block * k : block * (k + 1)]

    at = 0
    for w in (wg, wv, wk, wq):
        for c in range(0, w.shape[1], 256):
            put(at, jnp.dot(normed, w[:, c : c + 256], preferred_element_type=F32))
            at += 256
    heads = ws.shape[0]
    extra = lax.dot_general(normed, ws_s[...], NT, preferred_element_type=F32)
    put(at, with_squares(extra, squares, heads))


def with_squares(extra, squares, at):
    high, low = halves(squares)
    lane = lane_of(extra.shape)
    return jnp.where(lane == at, high, jnp.where(lane == at + 1, low, extra))


def project(tokens, gain, weights, near):
    seqs, prop, feat = tokens.shape
    columns = sum(w.shape[1] for w in weights[:4]) + LANES
    return pl.pallas_call(
        project_kernel,
        out_specs=[pl.BlockSpec(memory_space=VMEM)] * near,
        out_shape=[VMEM((seqs // near * prop, columns), BF16)] * near,
        scratch_shapes=[VMEM((seqs * prop, feat), F32), VMEM((LANES, feat), BF16)],
        name="project",
    )(tokens, gain.reshape(1, feat), *weights[:4], weights[4].T)


def fold_kernel(heads, order, *refs):
    *arrived, out = refs
    _, columns = arrived[0].shape
    _, prop, _ = out.shape
    for at in range(0, columns, LANES):
        total = arrived[0][:, at : at + LANES].astype(F32)
        for block in arrived[1:]:
            total = total + block[:, at : at + LANES].astype(F32)
        if at == columns - LANES:
            squares = total[:, heads : heads + 1] + total[:, heads + 1 : heads + 2]
            total = with_squares(total, squares, heads)
        for k, place in enumerate(order):
            out[k, :, at : at + LANES] = total[prop * place : prop * (place + 1)].astype(BF16)


def fold(arrived, order, heads):
    rows, columns = arrived[0].shape
    far = len(order)
    vmem = pl.BlockSpec(memory_space=VMEM)
    return pl.pallas_call(
        functools.partial(fold_kernel, heads, order),
        in_specs=[vmem] * len(arrived),
        out_specs=vmem,
        out_shape=VMEM((far, rows // far, columns), BF16),
        name="fold",
    )(*map(local, arrived))


def prepare_kernel(
    accepted,
    states,
    past_v,
    past_k,
    past_q,
    taps_v,
    taps_k,
    taps_q,
    bias,
    log_rate,
    out_gain,
    state,
    state_high,
    state_low,
    rows,
    base,
    taps,
    bias_out,
    rate,
    gain,
    sem,
):
    offset = accepted[0]
    fetch = pltpu.make_async_copy(states.at[0, pl.ds(offset, 1)], state, sem)
    fetch.start()
    span, prop = rows.shape[0], base.shape[0]
    at = 0
    for past, tap in ((past_v, taps_v), (past_k, taps_k), (past_q, taps_q)):
        width = past.shape[2]
        history = past[0].astype(F32)
        picked = history[0:span]
        for j in range(1, history.shape[0] - span + 1):
            picked = jnp.where(offset == j, history[j : j + span], picked)
        weight = tap[...].astype(F32)
        rows[:, at : at + width] = picked
        taps[:, at : at + width] = weight
        for t in range(prop):
            part = jnp.zeros((1, width), F32)
            for i in range(CONV):
                if t + i < span:
                    part = part + picked[t + i : t + i + 1] * weight[i : i + 1]
            base[t : t + 1, at : at + width] = part
        at += width
    bias_out[...] = bias[...]
    rate[...] = -jnp.exp(log_rate[...])
    gain[...] = out_gain[...]
    fetch.wait()
    for h in range(state.shape[1]):
        at = slice(h * state.shape[2], (h + 1) * state.shape[2])
        high = state[0, h].astype(BF16)
        state_high[at] = high
        state_low[at] = (state[0, h] - high.astype(F32)).astype(BF16)


def prepare(accepted, states, pasts, taps, bias, log_rate, out_gain):
    _, _, heads, head_dim, state_dim = states.shape
    inner = heads * head_dim
    width = sum(p.shape[2] for p in pasts)
    prop = pasts[0].shape[1] - (CONV - 1)
    plain, vmem = pl.BlockSpec(), pl.BlockSpec(memory_space=VMEM)
    return pl.pallas_call(
        prepare_kernel,
        in_specs=[pl.BlockSpec(memory_space=pltpu.SMEM), pl.BlockSpec(memory_space=pl.ANY), *[plain] * 9],
        out_specs=[vmem] * 9,
        out_shape=[
            VMEM((1, heads, head_dim, state_dim), F32),
            VMEM((inner, state_dim), BF16),
            VMEM((inner, state_dim), BF16),
            VMEM((CONV - 1, width), F32),
            VMEM((prop, width), F32),
            VMEM((CONV, width), F32),
            VMEM((1, heads), F32),
            VMEM((1, heads), F32),
            VMEM((1, inner), F32),
        ],
        scratch_shapes=[pltpu.SemaphoreType.DMA(())],
        name="prepare",
    )(
        accepted,
        states,
        *pasts,
        *taps,
        bias.reshape(1, heads),
        log_rate.reshape(1, heads),
        out_gain.reshape(1, inner),
    )


def chain_kernel(
    arrived, state_high, state_low, base, taps, bias, rate, gain, sent, moved_out, key_out, decay_out, new_out
):
    copies, prop, _ = arrived.shape
    inner, state_dim = state_high.shape
    heads = bias.shape[1]
    head_dim = inner // heads
    width = base.shape[1]
    kwidth = (width - inner) // 2
    groups = kwidth // state_dim
    per_group = inner // groups

    total = arrived[0].astype(F32)
    for i in range(1, copies):
        total = total + arrived[i].astype(F32)
    at_step = inner + width
    squares = total[:, at_step + heads : at_step + heads + 1] + total[:, at_step + heads + 1 : at_step + heads + 2]
    rscale = lax.rsqrt(squares / D + EPS)

    def scaled(start, stop):
        return (total[:, start:stop] * rscale).astype(BF16).astype(F32)

    new = scaled(inner, at_step)
    new_out[...] = new
    filtered = base[...] + new * taps[CONV - 1 : CONV]
    for i in range(1, CONV):
        later = jnp.concatenate([jnp.zeros((i, width), F32), new[: prop - i]], axis=0)
        filtered = filtered + later * taps[CONV - 1 - i : CONV - i]
    convolved = filtered / (1.0 + jnp.exp(-filtered))
    conv_v, conv_k, conv_q = convolved[:, :inner], convolved[:, inner : inner + kwidth], convolved[:, inner + kwidth :]

    raw = total[:, at_step : at_step + heads] * rscale + bias[...]
    steps = jnp.maximum(raw, 0.0) + jnp.log1p(jnp.exp(-jnp.abs(raw)))
    decay = jnp.exp(steps * rate[...])
    first_half = lane_of((prop, 2 * head_dim)) < head_dim

    def spread(x):
        return jnp.concatenate(
            [jnp.where(first_half, x[:, h : h + 1], x[:, h + 1 : h + 2]) for h in range(0, heads, 2)], axis=1
        )

    moved = spread(steps) * conv_v
    shrink = spread(decay)
    moved_out[0:prop, :] = moved
    moved_out[prop:, :] = jnp.zeros((moved_out.shape[0] - prop, inner), F32)
    key_out[...] = conv_k
    decay_out[...] = decay

    q_high, q_low = halves(conv_q)
    q_both = jnp.concatenate([q_high, q_low], axis=0).astype(BF16)
    row = lax.broadcasted_iota(jnp.int32, (prop, per_group), 0)
    ys = []
    for g in range(groups):
        cols = slice(g * per_group, (g + 1) * per_group)
        part = slice(g * state_dim, (g + 1) * state_dim)
        main = lax.dot_general(q_both[:, part], state_high[cols], NT, preferred_element_type=F32)
        rest = lax.dot_general(q_both[:prop, part], state_low[cols], NT, preferred_element_type=F32)
        carried = main[:prop] + main[prop:] + rest
        y = jnp.zeros((prop, per_group), F32)
        for t in range(prop):
            match = jnp.sum(conv_q[:, part] * conv_k[t : t + 1, part], axis=1, keepdims=True)
            carried = carried * shrink[t : t + 1, cols] + moved[t : t + 1, cols] * match
            y = jnp.where(row == t, carried, y)
        ys.append(y)
    y = jnp.concatenate(ys, axis=1)
    gate = scaled(0, inner)
    u = (y * (gate / (1.0 + jnp.exp(-gate))) * gain[...]).astype(BF16)
    for i in range(sent.shape[0]):
        sent[i] = u


def chain(copies, arrived, state_high, state_low, base, taps, bias, rate, gain):
    prop = arrived.shape[1]
    inner, heads, width = state_high.shape[0], bias.shape[1], base.shape[1]
    vmem = pl.BlockSpec(memory_space=VMEM)
    return pl.pallas_call(
        chain_kernel,
        in_specs=[vmem] * 8,
        out_specs=[vmem] * 5,
        out_shape=[
            VMEM((copies, prop, inner), BF16),
            VMEM((8, inner), F32),
            VMEM((prop, (width - inner) // 2), F32),
            VMEM((prop, heads), F32),
            VMEM((prop, width), F32),
        ],
        name="chain",
    )(*map(local, (arrived, state_high, state_low, base, taps, bias, rate, gain)))


def states_kernel(
    first, moved, keys, decay, rows, new, new_states, new_v, new_k, new_q, state_s, moved_s, sem_out
):
    prop, heads = decay.shape
    _, _, head_dim, state_dim = state_s.shape
    inner, kwidth = moved.shape[1], keys.shape[1]
    per_group = heads * state_dim // kwidth
    writes = []

    def write(source, slot):
        copy = pltpu.make_async_copy(source, new_states.at[0, slot], sem_out.at[slot])
        copy.start()
        writes.append(copy)

    write(first.at[0], 0)
    at = 0
    for out in (new_v, new_k, new_q):
        width = out.shape[2]
        both = jnp.concatenate([rows[:, at : at + width], new[:, at : at + width]], axis=0)
        out[0] = both.astype(BF16)
        at += width
    for c in range(0, inner, LANES):
        moved_s[c : c + LANES, :] = jnp.transpose(moved[:, c : c + LANES])
    for t in range(prop):
        for h in range(heads):
            g = h // per_group
            before = first[0, h] if t == 0 else state_s[t - 1, h]
            key_row = keys[t : t + 1, g * state_dim : (g + 1) * state_dim]
            column = moved_s[h * head_dim : (h + 1) * head_dim, t : t + 1]
            state_s[t, h] = before * decay[t : t + 1, h : h + 1] + column * key_row
        write(state_s.at[t], t + 1)
    for copy in writes:
        copy.wait()


def next_states(keep, first, moved, keys, decay, rows, new):
    _, heads, head_dim, state_dim = first.shape
    inner, kwidth = moved.shape[1], keys.shape[1]
    count = rows.shape[0] + new.shape[0]
    plain = pl.BlockSpec()
    vmem = pl.BlockSpec(memory_space=VMEM)
    return pl.pallas_call(
        states_kernel,
        in_specs=[vmem] * 6,
        out_specs=[pl.BlockSpec(memory_space=pl.ANY), plain, plain, plain],
        out_shape=[
            jax.ShapeDtypeStruct((1, keep, heads, head_dim, state_dim), F32),
            jax.ShapeDtypeStruct((1, count, inner), BF16),
            jax.ShapeDtypeStruct((1, count, kwidth), BF16),
            jax.ShapeDtypeStruct((1, count, kwidth), BF16),
        ],
        scratch_shapes=[
            VMEM((keep - 1, heads, head_dim, state_dim), F32),
            VMEM((inner, 8), F32),
            pltpu.SemaphoreType.DMA((keep,)),
        ],
        name="states",
    )(*map(local, (first, moved, keys, decay, rows, new)))


def output_kernel(blocks, w_out, gain, out):
    features = w_out.shape[0]
    x = blocks[...].reshape(-1, blocks.shape[2])
    out[:, :features] = lax.dot_general(x, w_out[...], NT, preferred_element_type=F32).astype(BF16)
    wide = x.astype(F32)
    inverse = 1.0 / (gain[...] * gain[...])
    squares = jnp.sum(wide * wide * inverse, axis=1, keepdims=True)
    high, low = halves(squares)
    lane = lane_of((x.shape[0], LANES - features))
    out[:, features:] = jnp.where(lane == 0, high, jnp.where(lane == 1, low, 0.0)).astype(BF16)


def output(rows, w_out, gain):
    vmem = pl.BlockSpec(memory_space=VMEM)
    return pl.pallas_call(
        output_kernel,
        in_specs=[vmem] * 3,
        out_specs=vmem,
        out_shape=VMEM((rows.shape[0] * rows.shape[1], LANES), BF16),
        name="output",
    )(local(rows), local(w_out.T), local(gain))


def combine_kernel(order, mine, other, out):
    _, prop, features = out.shape
    a, b = mine[...].astype(F32), other[...].astype(F32)
    squares_a = a[:, features : features + 1] + a[:, features + 1 : features + 2]
    squares_b = b[:, features : features + 1] + b[:, features + 1 : features + 2]
    scale = lax.rsqrt((squares_a + squares_b) / WIDTH + EPS)
    mixed = (a[:, :features] + b[:, :features]) * scale
    for i, seq in enumerate(order):
        out[seq] = mixed[prop * i : prop * (i + 1)].astype(BF16)


def combine(mine, other, order, features):
    seqs = len(order)
    vmem = pl.BlockSpec(memory_space=VMEM)
    return pl.pallas_call(
        functools.partial(combine_kernel, order),
        in_specs=[vmem, vmem],
        out_shape=jax.ShapeDtypeStruct((seqs, mine.shape[0] // seqs, features), BF16),
        name="combine",
    )(local(mine), local(other))


def per_device(
    tokens,
    in_gain,
    w_gate,
    w_value,
    w_key,
    w_query,
    w_step,
    conv_value,
    conv_key,
    conv_query,
    step_bias,
    decay_log,
    out_gain,
    w_out,
    past_value,
    past_key,
    past_query,
    past_states,
    accepted,
):
    group_seqs, _, features = tokens.shape
    near, far = lax.axis_size("ky"), lax.axis_size("kz")
    far_order = [(far // 2 + 1 + i) % far for i in range(far)]
    order = [(far // 2 + i) % far * near + (near // 2 + j) % near for j in range(near) for i in range(far)]
    weights = (w_gate, w_value, w_key, w_query, w_step)
    own, *others = project(tokens, in_gain, weights, near)
    nearby = {0: own}
    for k in sorted(range(1, near), key=lambda k: -min(k, near - k)):
        nearby[k] = lax.ppermute(others[k - 1], "ky", [(i, (i + k) % near) for i in range(near)])
    first, high, low, rows, base, taps, bias, rate, gain = prepare(
        accepted,
        past_states,
        (past_value, past_key, past_query),
        (conv_value, conv_key, conv_query),
        step_bias,
        decay_log,
        out_gain,
    )
    partial = fold([nearby[k] for k in range(near)], far_order, w_step.shape[1])
    arrived = lax.all_to_all(partial, "kz", 0, 0, axis_index_groups=[far_order], tiled=True)
    sent, moved, keys, decay, new = chain(group_seqs, arrived, high, low, base, taps, bias, rate, gain)
    gathered = lax.all_to_all(sent, KV, 0, 0, axis_index_groups=[order], tiled=True)
    saved = next_states(past_states.shape[1], first, moved, keys, decay, rows, new)
    mine = output(gathered, w_out, gain)
    swap = [(i, 1 - i) for i in range(2)]
    mixed = combine(mine, lax.ppermute(mine, "tp", swap), order, features)
    return (mixed, *saved)


def solution(mesh):
    dp, kv, tp = mesh.devices.shape
    near = NEAR if kv % NEAR == 0 else 1
    split = jax.sharding.Mesh(mesh.devices.reshape(dp, kv // near, near, tp), ("dp", *KV, "tp"))
    placed = (
        P("dp", None, KV),
        P(KV),
        P(KV, "tp"),
        P(KV, "tp"),
        P(KV, "tp"),
        P(KV, "tp"),
        P(KV, "tp"),
        P(None, "tp"),
        P(None, "tp"),
        P(None, "tp"),
        P("tp"),
        P("tp"),
        P("tp"),
        P("tp", KV),
        P(("dp", *KV), None, "tp"),
        P(("dp", *KV), None, "tp"),
        P(("dp", *KV), None, "tp"),
        P(("dp", *KV), None, "tp", None, None),
        P(("dp", *KV)),
    )
    return jax.shard_map(
        per_device,
        mesh=split,
        in_specs=placed,
        out_specs=(
            P("dp", None, KV),
            P(("dp", *KV), None, "tp", None, None),
            P(("dp", *KV), None, "tp"),
            P(("dp", *KV), None, "tp"),
            P(("dp", *KV), None, "tp"),
        ),
        check_vma=False,
    )
```
